32 devices in a mesh: fs: 8 (over z, y), tp: 4 (over x, core).
Axes of the slice: x: 2, y: 2, z: 4, core: 2. Of those that a mesh axis runs over, the one named last changes fastest.
Arguments:
- tokens: bfloat16 [3072, 2048], P('tp'), may hold values from -6 to 6
- norm_gain: float32 [2048], P('fs'), may hold values from 0.1 to 1.9
- gate_weight: float32 [4, 2048, 8192], P(None, 'fs', 'tp'), may hold values from -0.125 to 0.125
- up_weight: float32 [4, 2048, 8192], P(None, 'fs', 'tp'), may hold values from -0.125 to 0.125
- down_weight: float32 [4, 8192, 2048], P(None, 'fs', 'tp'), may hold values from -0.0625 to 0.0625
- routes: int32 [3072, 2], P('tp'), may hold values from 0 to 3, all different within a row; in each aligned block of 768 rows (0 to 767, 768 to 1535, ...) at most 480 rows name the same one
- route_logit: float32 [3072, 2], P('tp'), may hold values from -6 to 6
Outputs:
- gate_out: bfloat16 [4, 2048, 8192], P(None, None, 'fs')
- up_out: bfloat16 [4, 2048, 8192], P(None, None, 'fs')
- down_out: bfloat16 [4, 8192, 2048], P(None, 'fs')
- mixed: bfloat16 [3072, 2048], P(('tp', 'fs'))
The draws below stay inside these ranges and needn't reach their ends.
Inputs may be any that keep to these rules, and one draw needn't show every extreme that they name: `routes`: the two experts of a token differ. In each aligned block of 768 tokens (the tokens of one request group) every expert is named by at most 480 tokens, a bound that some block reaches.
All inputs are finite; a program needn't handle non-finite values.
Results may differ from the reference program's by a relative error of at most 0.0082.
Values may be sent and summed in bfloat16 or wider, within the bound.
A program may use at most 192 MiB of HBM per device.

```python
import math
import jax
import jax.numpy as jnp
import numpy as np
from jax import lax

D = 2048
FF = 8192
E = 4
TOK_GROUP = 768
CAP = 480
TOKENS = 3072


def levels(stream_key, dims, shards, least, largest):
    factor_of = 1.0
    for axis_at, parts in shards:
        steps = jax.random.uniform(jax.random.fold_in(jax.random.fold_in(stream_key, 6), axis_at), (parts,), jnp.float32, least / len(shards), largest / len(shards))
        factor_of = factor_of * jnp.repeat(jnp.exp(steps), dims[axis_at] // parts).reshape((-1,) + (1,) * (len(dims) - 1 - axis_at))
    return factor_of


def deal_out(rng, own, number, rows, number_of, top, limit, skew):
    sequence = jax.random.permutation(rng, number_of)
    packed, ordinary = load_shares(number_of, rows * top, limit, skew, True), load_shares(number_of, rows * top, limit, skew, False)
    places = jnp.arange(number_of)

    def named(tallies, rotation):
        used = int((tallies > 0).sum())
        fixed = max(1, used // 4)
        passed = fixed + (places - fixed + rotation * (used - fixed)) % max(1, number_of - fixed)
        return jnp.zeros((number_of,), jnp.int32).at[sequence[jnp.where(places < fixed, places, passed)]].set(jnp.asarray(tallies, jnp.int32))

    tallies = jnp.where(number % 4 == 0, named(packed, number // 4), named(ordinary, number - number // 4 - 1))
    mixed = jax.random.permutation(jax.random.fold_in(own, 3), number_of)
    source_of, receiver = mixed[0:number_of // 2 * 2:2], mixed[1:number_of // 2 * 2:2]
    margin = jnp.minimum(tallies[source_of] - 1, limit - tallies[receiver]) // 2
    margin = jnp.where((source_of == sequence[0]) | (receiver == sequence[0]) | (tallies[receiver] == 0), 0, jnp.maximum(margin, 0))
    passed = jax.random.randint(jax.random.fold_in(own, 4), (number_of // 2,), 0, 1 << 20) % (margin + 1)
    tallies = tallies.at[source_of].add(-passed).at[receiver].add(passed)
    items = jnp.searchsorted(jnp.cumsum(tallies), jnp.arange(rows * top), side="right").astype(jnp.int32)
    grid = items.reshape(top, rows).T
    grid = grid[jax.random.permutation(jax.random.fold_in(own, 1), rows)]
    rotation = jax.random.randint(jax.random.fold_in(own, 2), (rows, 1), 0, top)
    return jnp.take_along_axis(grid, (jnp.arange(top)[None, :] + rotation) % top, axis=1)


def load_shares(amount, total, bound, skew, full):
    loads = [(1 << 20) // math.isqrt(grade ** skew) + 1 for grade in range(1, amount + 1)]
    largest = bound if full else min(bound, max(-(-total // amount), total * loads[0] // sum(loads)))
    least = 1 if total - largest >= amount - 1 else 0
    counts, spare = [largest] + [least] * (amount - 1), total - largest - least * (amount - 1)
    while spare > 0:
        movable = [i for i in range(1, amount) if counts[i] < largest] or [i for i in range(1, amount) if counts[i] < bound]
        pool, left = sum([loads[i] for i in movable]), spare
        for i in movable:
            more = min(bound - counts[i], max(1, left * loads[i] // pool), spare)
            counts[i] = counts[i] + more
            spare = spare - more
    return np.array(counts)


def scatter_about(stream_key, shape, deviation, limit, pieces=(), held_as=jnp.bfloat16):
    entries = jax.random.normal(stream_key, shape, jnp.float32) * deviation
    if len(pieces) > 0:
        entries = levels(stream_key, shape, pieces, -0.22, 0.18) * entries
    return jnp.clip(entries, min=-limit, max=limit).astype(held_as)


def setup_inputs(seed: int = 0) -> dict:
    seeds = jax.random.split(jax.random.key(seed), 8)
    tokens = scatter_about(seeds[0], (TOKENS, D), 1.0, 6.0, ((0, 4),))
    norm_gain = jnp.clip(1.0 + 0.18 * jax.random.normal(seeds[1], (D,), jnp.float32), 0.1, 1.9)
    gate_weight = scatter_about(seeds[2], (E, D, FF), D ** -0.5, 0.125, ((1, 8), (2, 4)), jnp.float32)
    up_weight = scatter_about(seeds[3], (E, D, FF), D ** -0.5, 0.125, ((1, 8), (2, 4)), jnp.float32)
    down_weight = scatter_about(seeds[4], (E, FF, D), FF ** -0.5, 0.0625, ((1, 8), (2, 4)), jnp.float32)
    routes_keys = jax.random.split(jax.random.fold_in(seeds[5], 1), TOKENS // TOK_GROUP)
    routes_turns = jax.random.permutation(jax.random.fold_in(seeds[5], 3), TOKENS // TOK_GROUP)
    routes = jax.vmap(lambda own, number: deal_out(jax.random.fold_in(seeds[5], 2), own, number, TOK_GROUP, E, 2, CAP, 1))(routes_keys, routes_turns).reshape((TOKENS, 2))
    route_logit = scatter_about(seeds[6], (TOKENS, 2), 1.0, 6.0, ((0, 4),), jnp.float32)
    return dict(tokens=tokens, norm_gain=norm_gain, gate_weight=gate_weight, up_weight=up_weight, down_weight=down_weight, routes=routes, route_logit=route_logit)


EPS = 0.5

def reference(tokens, norm_gain, gate_weight, up_weight, down_weight, routes, route_logit):
    gain_col = norm_gain.astype(jnp.float32)[None, :, None]
    gate_out = (gate_weight * gain_col).astype(jnp.bfloat16)
    up_out = (up_weight * gain_col).astype(jnp.bfloat16)
    down_out = down_weight.astype(jnp.bfloat16)
    floats = tokens.astype(jnp.float32)
    normed = (floats * lax.rsqrt(lax.optimization_barrier(jnp.mean(floats * floats, axis=1, keepdims=True)) + EPS)).astype(jnp.bfloat16)
    first_share = jax.nn.sigmoid(route_logit[:, 0] - route_logit[:, 1])
    shares = jnp.stack([first_share, 1.0 - first_share], axis=1)
    summed = jnp.zeros(tokens.shape, jnp.float32)
    for expert in range(E):
        weight_col = lax.optimization_barrier(jnp.sum(jnp.where(routes == expert, shares, 0.0), axis=1, keepdims=True))
        gate_val = jnp.dot(normed, gate_out[expert], preferred_element_type=jnp.float32)
        up_val = jnp.dot(normed, up_out[expert], preferred_element_type=jnp.float32)
        hidden = (jax.nn.silu(gate_val) * up_val).astype(jnp.bfloat16)
        result = jnp.dot(hidden, down_out[expert], preferred_element_type=jnp.float32)
        summed = summed + weight_col * result
    return (gate_out, up_out, down_out, summed.astype(jnp.bfloat16))
```

```python
import functools

import jax
import jax.numpy as jnp
from jax import lax
from jax.experimental import pallas as pl
from jax.experimental.pallas import tpu as pltpu
from jax.sharding import PartitionSpec as P

EPS = 0.5
MESH = pl.DeviceIdType.MESH
VMEM_LIMIT = 63 * 1024 * 1024


def expert_rows(x, weight, wide, tall, total, expert):
    rows = x.shape[0]
    tile = rows // 2

    def step(i, carry):
        at = pl.ds(pl.multiple_of(i * tile, tile), tile)
        mine = x[at, :]
        gate_val = jnp.dot(mine, wide[0], preferred_element_type=jnp.float32)
        up_val = jnp.dot(mine, wide[1], preferred_element_type=jnp.float32)
        hidden = (jax.nn.silu(gate_val) * up_val).astype(jnp.bfloat16)
        result = jnp.dot(hidden, tall[...], preferred_element_type=jnp.float32)
        shares = weight[at, :]
        lane = lax.broadcasted_iota(jnp.int32, shares.shape, 1)
        share = jnp.sum(jnp.where(lane == expert, shares, 0.0), axis=1, keepdims=True)
        total[at, :] += share * result
        return carry

    lax.fori_loop(0, rows // tile, step, 0)


def spread(
    cuts, special,
    gain, tokens, routes, logit, gate_f32, up_f32, down_f32,
    gate_all, up_all, down_all, x_out, weight_out, total_out,
    own, far, down, stage, down_stage, x, weight, total, wide, tall,
    load, across_send, across_recv, near_send, near_recv, far_send, twin_send, twin_recv,
    onward_send, down_send, down_recv, local_sem, fetch_sem,
):
    _, blocks, depth, both = own.shape
    experts = blocks // cuts
    features, units = gate_all.shape[1:]
    block = units // cuts
    per = both // block
    fs, tp = lax.axis_index("fs"), lax.axis_index("tp")
    half, side = tp // 2, tp % 2
    twin = half * 2 + 1 - side
    col = down.shape[2]
    group = fs // per
    relay_side = group % 2
    lands = side != relay_side
    beyond = (1 - half) * 2
    apart = group // 2 != half
    close = group // 2 == half
    full = (gate_all, up_all)

    def remote(src, dst, send, recv, fs_to, tp_to):
        return pltpu.make_async_remote_copy(
            src_ref=src, dst_ref=dst, send_sem=send, recv_sem=recv,
            device_id=(fs_to, tp_to), device_id_type=MESH,
        )

    def columns(owner):
        return pl.ds(pl.multiple_of(owner * col, col), col)

    def slab(v):
        return v // cuts, pl.ds(pl.multiple_of(v % cuts * block, block), block)

    def only(condition, needed, action):
        if needed:
            pl.when(condition)(action)
        else:
            action()

    pieces = [(a, v) for v in range(blocks) for a in range(2)]
    early, late = pieces[:special], pieces[special : 2 * special]
    rows = pl.ds(pl.multiple_of(fs * depth, depth), depth)

    def crossing(a, v):
        return remote(
            own.at[a, v], far.at[side, a, v], across_send.at[a, v], across_recv.at[side, a, v],
            fs, beyond + relay_side,
        )

    def deal(source, a, v, owner, sem):
        e, at = slab(v)
        for h in range(per):
            remote(
                source.at[:, pl.ds(h * block, block)],
                full[a].at[e, rows, at],
                sem,
                near_recv.at[a, v],
                owner * per + h,
                half * 2 + 1 - owner % 2,
            ).start()

    def fetch(n):
        a, v = pieces[n]
        for h in range(per):
            pltpu.make_async_copy(
                (gate_f32, up_f32)[a].at[
                    v // cuts, :, pl.ds(h * units + v % cuts * block, block)
                ],
                stage.at[n % 2, :, pl.ds(h * block, block)],
                load.at[n % 2],
            ).start()

    def fetched(n):
        pltpu.make_async_copy(stage.at[n % 2], stage.at[n % 2], load.at[n % 2]).wait()

    def fetch_down(e):
        return pltpu.make_async_copy(down_f32.at[e], down_stage.at[e % 2], load.at[2 + e % 2])

    def down_local(e):
        return pltpu.make_async_copy(
            down.at[e], down_all.at[e, :, columns(tp)], local_sem.at[4 + e]
        )

    def down_to(k, e):
        return remote(
            down.at[e], down_all.at[e, :, columns(tp)], down_send.at[k, e],
            down_recv.at[(0, 1 + side)[k], e], fs, (twin, beyond + relay_side)[k],
        )

    def down_pass(s, e):
        part = down_all.at[e, :, columns(beyond + s)]
        return remote(part, part, down_send.at[2 + s, e], down_recv.at[1 + s, e], fs, twin)

    tile = min(depth, 32)
    fetch(0)
    token_copy = pltpu.make_async_copy(tokens, x, local_sem.at[0])
    token_copy.start()
    spot = lax.broadcasted_iota(jnp.int32, (depth, depth), 0)
    lane = lax.broadcasted_iota(jnp.int32, (depth, depth), 1)
    factor = jnp.sum(jnp.where(spot == lane, gain[...], 0.0), axis=1, keepdims=True)
    weight[0:depth, :] = jnp.broadcast_to(factor, (depth, weight.shape[1]))
    for n, piece in enumerate(pieces):
        a, v = piece
        if n + 1 < len(pieces):
            fetch(n + 1)
        e = v // cuts
        if a == 0 and v % cuts == 0:
            fetch_down(e).start()
        fetched(n)

        def scale(i, carry, a=a, v=v, n=n):
            at = pl.ds(pl.multiple_of(i * tile, tile), tile)
            own[a, v, at, :] = (stage[n % 2, at, :] * weight[at, 0:1]).astype(own.dtype)
            return carry

        lax.fori_loop(0, depth // tile, scale, 0)
        only(close, piece in late, lambda: crossing(a, v).start())
        only(close, piece in early, lambda: deal(own.at[a, v], a, v, tp, near_send.at[a, v]))
        if a == 1 and v % cuts == cuts - 1:
            fetch_down(e).wait()
            short = min(units, 128)

            def narrow(i, carry, e=e):
                at = pl.ds(pl.multiple_of(i * short, short), short)
                down[e, at, :] = down_stage[e % 2, at, :].astype(down.dtype)
                return carry

            lax.fori_loop(0, units // short, narrow, 0)
            down_to(1, e).start()
            down_to(0, e).start()
            down_local(e).start()

    token_copy.wait()
    count = x.shape[0]
    strip = count // 8

    def normalise(i, carry):
        at = pl.ds(pl.multiple_of(i * strip, strip), strip)
        floats = x[at, :].astype(jnp.float32)
        x[at, :] = (
            floats * lax.rsqrt(jnp.mean(floats * floats, axis=1, keepdims=True) + EPS)
        ).astype(x.dtype)
        return carry

    lax.fori_loop(0, count // strip, normalise, 0)
    first = jax.nn.sigmoid(logit[0:1, :] - logit[1:2, :])
    expert_of = lax.broadcasted_iota(jnp.int32, (weight.shape[1], count), 0)
    by_expert = jnp.where(routes[0:1, :] == expert_of, first, 0.0) + jnp.where(
        routes[1:2, :] == expert_of, 1.0 - first, 0.0
    )
    weight[...] = by_expert.T
    total[...] = jnp.zeros_like(total)
    x_copy = pltpu.make_async_copy(x, x_out, local_sem.at[1])
    x_copy.start()
    weight_copy = pltpu.make_async_copy(weight, weight_out, local_sem.at[2])
    weight_copy.start()

    def relay(a, v):
        for s in range(2):
            part = far.at[s, a, v]
            pltpu.make_async_copy(part, part, across_recv.at[s, a, v]).wait()
            deal(part, a, v, beyond + s, far_send.at[s, a, v])

    def relay_down(e):
        for s in range(2):
            down_pass(s, e).wait_recv()
            down_pass(s, e).start()

    away = pl.ds(pl.multiple_of((1 - group // 2) * (features // 2), features // 2), features // 2)

    def hand(a, v):
        e, at = slab(v)
        part = full[a].at[e, :, at]
        return remote(part, part, twin_send.at[a, v], twin_recv.at[a, v], fs, twin)

    def onward(a, v):
        e, at = slab(v)
        part = full[a].at[e, away, at]
        return remote(part, part, onward_send.at[a, v], near_recv.at[a, v], fs, beyond + side)

    def take(a, v, forward):
        e, at = slab(v)
        part = full[a].at[e, :, at]
        pltpu.make_async_copy(part, part, near_recv.at[a, v]).wait()
        if forward:
            onward(a, v).start()
        hand(a, v).start()

    def take_all(group_of, forward):
        for a, v in group_of:
            take(a, v, forward)

    @pl.when(jnp.logical_not(lands))
    def _():
        for a, v in pieces[: 2 * special]:
            only(apart, (a, v) in late, functools.partial(relay, a, v))
            if a == 1 and v % cuts == cuts - 1:
                relay_down(v // cuts)

        def pass_on(v, carry):
            relay(0, v)
            relay(1, v)
            pl.when(v % cuts == cuts - 1)(lambda: relay_down(v // cuts))
            return carry

        lax.fori_loop(special, blocks, pass_on, 0)

    @pl.when(lands)
    def _():
        pl.when(close)(lambda: take_all(late, True))
        pl.when(apart)(lambda: take_all(early, True))

    def arrive(v):
        @pl.when(lands)
        def _():
            take(0, v, False)
            take(1, v, False)

        @pl.when(jnp.logical_not(lands))
        def _():
            hand(0, v).wait_recv()
            hand(1, v).wait_recv()

    def down_ready(e):
        down_local(e).wait()
        down_to(0, e).wait_recv()

        @pl.when(lands)
        def _():
            for s in range(2):
                down_pass(s, e).wait_recv()

    def compute(v):
        e, at = slab(v)
        copies = [
            pltpu.make_async_copy(gate_all.at[e, :, at], wide.at[0], fetch_sem.at[0]),
            pltpu.make_async_copy(up_all.at[e, :, at], wide.at[1], fetch_sem.at[1]),
            pltpu.make_async_copy(down_all.at[e, at, :], tall, fetch_sem.at[2]),
        ]
        for copy in copies:
            copy.start()
        for copy in copies:
            copy.wait()
        expert_rows(x, weight, wide, tall, total, e)

    for e in range(special // cuts):
        down_ready(e)

    def turn(v, carry):
        arrive(v)
        pl.when(jnp.logical_or(v % cuts == 0, v == special))(lambda: down_ready(v // cuts))
        compute(v)
        return carry

    lax.fori_loop(special, blocks - 1, turn, 0)
    total_copy = pltpu.make_async_copy(total, total_out, local_sem.at[3])
    total_copy.start()
    if (blocks - 1) // cuts != (blocks - 2) // cuts:
        down_ready(experts - 1)

    @pl.when(lands)
    def _():
        take_all(pieces[-2:], False)
        pl.when(close)(lambda: take_all(early, False))
        pl.when(apart)(lambda: take_all(late, False))
        for a, v in pieces:
            hand(a, v).wait_send()

        def sent(group_of):
            for a, v in group_of:
                onward(a, v).wait_send()

        pl.when(close)(lambda: sent(late))
        pl.when(apart)(lambda: sent(early))

    @pl.when(jnp.logical_not(lands))
    def _():
        for a, v in pieces[: 2 * special] + pieces[-2:]:
            hand(a, v).wait_recv()
        for s in range(2):
            for a, v in pieces:
                gone = functools.partial(
                    pltpu.make_async_copy, far.at[s, a, v], far.at[s, a, v], far_send.at[s, a, v]
                )
                only(apart, (a, v) in late, lambda gone=gone: gone().wait())
            for e in range(experts):
                down_pass(s, e).wait_send()

    for piece in pieces:
        a, v = piece

        def dealt(sem, a=a, v=v):
            pltpu.make_async_copy(own.at[a, v], own.at[a, v], sem).wait()

        only(close, piece in late, lambda: crossing(a, v).wait_send())
        only(close, piece in early, lambda: dealt(near_send.at[a, v]))
    for e in range(experts):
        down_to(0, e).wait_send()
        down_to(1, e).wait_send()
    x_copy.wait()
    weight_copy.wait()
    total_copy.wait()


def finish(
    cuts, special,
    gate_all, up_all, down_all, x_in, weight_in, total_in,
    gate_out, up_out, down_out, part,
    wide, tall, x, weight, total, take_sem, put_sem, side_sem,
):
    slots = wide.shape[0]
    units = gate_all.shape[2]
    block = units // cuts
    blocks = gate_all.shape[0] * cuts
    turns = blocks // 2

    def place(s):
        i = s // 2
        mine = jnp.where(i == turns - 1, blocks - 1, i)
        v = jnp.where(s % 2 == 0, mine, special + i)
        return v // cuts, pl.ds(pl.multiple_of(v % cuts * block, block), block)

    def pull(s):
        e, at = place(s)
        slot = s % slots
        return [
            pltpu.make_async_copy(gate_all.at[e, :, at], wide.at[slot, 0], take_sem.at[slot, 0]),
            pltpu.make_async_copy(up_all.at[e, :, at], wide.at[slot, 1], take_sem.at[slot, 1]),
            pltpu.make_async_copy(down_all.at[e, at, :], tall.at[slot], take_sem.at[slot, 2]),
        ]

    def push(s):
        e, at = place(s)
        slot = s % slots
        return [
            pltpu.make_async_copy(wide.at[slot, 0], gate_out.at[e, :, at], put_sem.at[slot, 0]),
            pltpu.make_async_copy(wide.at[slot, 1], up_out.at[e, :, at], put_sem.at[slot, 1]),
            pltpu.make_async_copy(tall.at[slot], down_out.at[e, at, :], put_sem.at[slot, 2]),
        ]

    def start(copies):
        for copy in copies:
            copy.start()

    def wait(copies):
        for copy in copies:
            copy.wait()

    sides = [
        pltpu.make_async_copy(x_in, x, side_sem.at[0]),
        pltpu.make_async_copy(weight_in, weight, side_sem.at[1]),
        pltpu.make_async_copy(total_in, total, side_sem.at[2]),
    ]
    start(pull(0))
    start(sides)
    start(pull(1))
    wait(sides)

    def turn(i, carry):
        for s in (2 * i, 2 * i + 1):
            wait(pull(s))
            start(push(s))

        @pl.when(i >= 1)
        def _():
            wait(push(2 * i - 2))
            wait(push(2 * i - 1))

        @pl.when(i + 1 < turns)
        def _():
            start(pull(2 * i + 2))
            start(pull(2 * i + 3))

        slot = 2 * i % slots
        expert_rows(x, weight, wide.at[slot], tall.at[slot], total, place(2 * i)[0])
        return carry

    lax.fori_loop(0, turns, turn, 0)
    part[...] = total[...].astype(part.dtype)
    wait(push(blocks - 2))
    wait(push(blocks - 1))


def fold(chunks, part, out, low_in, mid, high_in, low_send, low_recv, high_send, high_recv):
    highs, _, rows, width = part.shape
    step = width // chunks
    fs, tp = lax.axis_index("fs"), lax.axis_index("tp")
    high, low = fs // 2, fs % 2
    first = []
    for k in range(chunks):
        copy = pltpu.make_async_remote_copy(
            src_ref=part.at[:, 1 - low, :, pl.ds(k * step, step)],
            dst_ref=low_in.at[k],
            send_sem=low_send.at[k],
            recv_sem=low_recv.at[k],
            device_id=(high * 2 + 1 - low, tp),
            device_id_type=MESH,
        )
        copy.start()
        first.append(copy)
    second = []
    for k in range(chunks):
        first[k].wait_recv()
        mid[k] = (
            part[:, low, :, pl.ds(k * step, step)].astype(jnp.float32)
            + low_in[k].astype(jnp.float32)
        ).astype(mid.dtype)
        for shift in range(1, highs):
            to = lax.rem(high + shift, highs)
            copy = pltpu.make_async_remote_copy(
                src_ref=mid.at[k, to],
                dst_ref=high_in.at[k, shift],
                send_sem=high_send.at[k, shift],
                recv_sem=high_recv.at[k, shift],
                device_id=(to * 2 + low, tp),
                device_id_type=MESH,
            )
            copy.start()
            second.append((k, copy))
    for k in range(chunks):
        total = part[high, low, :, pl.ds(k * step, step)].astype(jnp.float32) + low_in[
            k, high
        ].astype(jnp.float32)
        shift = 0
        for at, copy in second:
            if at == k:
                shift += 1
                copy.wait_recv()
                total = total + high_in[k, shift].astype(jnp.float32)
        out[:, pl.ds(k * step, step)] = total.astype(out.dtype)
    for copy in first:
        copy.wait_send()
    for _, copy in second:
        copy.wait_send()


def shards(fs_size, tokens, norm_gain, gate_weight, up_weight, down_weight, routes, route_logit):
    experts, depth, width = gate_weight.shape
    _, units, col = down_weight.shape
    rows, features = tokens.shape
    half = jnp.bfloat16
    anywhere = pl.BlockSpec(memory_space=pl.ANY)
    vmem = pl.BlockSpec(memory_space=pltpu.VMEM)
    dma = pltpu.SemaphoreType.DMA
    block = min(units, 512)
    cuts = units // block
    blocks = experts * cuts
    special = blocks // 2 - 1
    both = width // cuts
    gate_shape = jax.ShapeDtypeStruct((experts, features, units), half)
    down_shape = jax.ShapeDtypeStruct((experts, units, features), half)
    gate_all, up_all, down_all, x, weight, total = pl.pallas_call(
        functools.partial(spread, cuts, special),
        out_shape=(
            gate_shape, gate_shape, down_shape,
            jax.ShapeDtypeStruct((rows, features), half),
            jax.ShapeDtypeStruct((rows, 128), jnp.float32),
            jax.ShapeDtypeStruct((rows, features), jnp.float32),
        ),
        in_specs=[vmem, anywhere, vmem, vmem] + [anywhere] * 3,
        out_specs=(anywhere,) * 6,
        scratch_shapes=[
            pltpu.VMEM((2, blocks, depth, both), half),
            pltpu.VMEM((2, 2, blocks, depth, both), half),
            pltpu.VMEM((experts, units, col), half),
            pltpu.VMEM((2, depth, both), jnp.float32),
            pltpu.VMEM((2, units, col), jnp.float32),
            pltpu.VMEM((rows, features), half),
            pltpu.VMEM((rows, 128), jnp.float32),
            pltpu.VMEM((rows, features), jnp.float32),
            pltpu.VMEM((2, features, block), half),
            pltpu.VMEM((block, features), half),
            dma((4,)),
        ]
        + [dma((2, blocks)), dma((2, 2, blocks))]
        + [dma((2, blocks))] * 2
        + [dma((2, 2, blocks))]
        + [dma((2, blocks))] * 3
        + [dma((4, experts)), dma((3, experts))]
        + [dma((4 + experts,)), dma((3,))],
        compiler_params=pltpu.CompilerParams(
            has_side_effects=True, vmem_limit_bytes=VMEM_LIMIT
        ),
        name="spread",
    )(norm_gain[None, :], tokens, routes.T, route_logit.T, gate_weight, up_weight, down_weight)

    gate_out, up_out, down_out, part = pl.pallas_call(
        functools.partial(finish, cuts, special),
        out_shape=(
            gate_shape, gate_shape, down_shape, jax.ShapeDtypeStruct((rows, features), half),
        ),
        in_specs=[anywhere] * 6,
        out_specs=(anywhere,) * 3 + (vmem,),
        scratch_shapes=[
            pltpu.VMEM((4, 2, features, block), half),
            pltpu.VMEM((4, block, features), half),
            pltpu.VMEM((rows, features), half),
            pltpu.VMEM((rows, 128), jnp.float32),
            pltpu.VMEM((rows, features), jnp.float32),
            dma((4, 3)), dma((4, 3)), dma((3,)),
        ],
        compiler_params=pltpu.CompilerParams(vmem_limit_bytes=VMEM_LIMIT),
        name="finish",
    )(gate_all, up_all, down_all, x, weight, total)

    highs, mine, chunks = fs_size // 2, rows // fs_size, 8
    step = features // chunks
    mixed = pl.pallas_call(
        functools.partial(fold, chunks),
        out_shape=jax.ShapeDtypeStruct((mine, features), half),
        in_specs=[vmem],
        out_specs=vmem,
        scratch_shapes=[pltpu.VMEM((chunks, highs, mine, step), half)] * 3
        + [dma((chunks,))] * 2
        + [dma((chunks, highs))] * 2,
        compiler_params=pltpu.CompilerParams(
            has_side_effects=True, vmem_limit_bytes=VMEM_LIMIT // 2
        ),
        name="fold",
    )(part.reshape(highs, 2, mine, features))
    return (gate_out, up_out, down_out, mixed)


def solution(mesh):
    return jax.shard_map(
        functools.partial(shards, mesh.shape["fs"]),
        mesh=mesh,
        in_specs=(
            P("tp", None),
            P("fs"),
            P(None, "fs", "tp"),
            P(None, "fs", "tp"),
            P(None, "fs", "tp"),
            P("tp", None),
            P("tp", None),
        ),
        out_specs=(
            P(None, None, "fs"),
            P(None, None, "fs"),
            P(None, "fs", None),
            P(("tp", "fs"), None),
        ),
        check_vma=False,
    )
```

```python
import functools

import jax
import jax.numpy as jnp
from jax import lax
from jax.experimental import pallas as pl
from jax.experimental.pallas import tpu as pltpu
from jax.sharding import PartitionSpec as P

EPS = 0.5
MESH = pl.DeviceIdType.MESH
VMEM_LIMIT = 63 * 1024 * 1024


def expert_tile(x, weight, wide, tall, total, expert, at):
    mine = x[at, :]
    gate_val = jnp.dot(mine, wide[0], preferred_element_type=jnp.float32)
    up_val = jnp.dot(mine, wide[1], preferred_element_type=jnp.float32)
    hidden = (jax.nn.silu(gate_val) * up_val).astype(jnp.bfloat16)
    result = jnp.dot(hidden, tall[...], preferred_element_type=jnp.float32)
    shares = weight[at, :]
    lane = lax.broadcasted_iota(jnp.int32, shares.shape, 1)
    share = jnp.sum(jnp.where(lane == expert, shares, 0.0), axis=1, keepdims=True)
    total[at, :] += share * result


def expert_rows(x, weight, wide, tall, total, expert):
    rows = x.shape[0]
    tile = rows // 2

    def step(i, carry):
        at = pl.ds(pl.multiple_of(i * tile, tile), tile)
        expert_tile(x, weight, wide, tall, total, expert, at)
        return carry

    lax.fori_loop(0, rows // tile, step, 0)


def spread(
    cuts, special,
    gain, tokens, routes, logit, gate_f32, up_f32, down_f32,
    gate_all, up_all, down_all, far, mixed,
    own, down, stage, down_stage, x, weight, total, wide, tall, part, low_in, mid, high_in,
    load, across_send, across_recv, near_send, near_recv, far_send, twin_send, twin_recv,
    onward_send, down_send, down_recv, local_sem, fetch_sem,
    low_send, low_recv, high_send, high_recv,
):
    _, blocks, depth, both = own.shape
    experts = blocks // cuts
    features, units = gate_all.shape[1:]
    block = units // cuts
    per = both // block
    fs, tp = lax.axis_index("fs"), lax.axis_index("tp")
    half, side = tp // 2, tp % 2
    twin = half * 2 + 1 - side
    col = down.shape[2]
    group = fs // per
    relay_side = group % 2
    lands = side != relay_side
    beyond = (1 - half) * 2
    apart = group // 2 != half
    close = group // 2 == half
    full = (gate_all, up_all)

    def remote(src, dst, send, recv, fs_to, tp_to):
        return pltpu.make_async_remote_copy(
            src_ref=src, dst_ref=dst, send_sem=send, recv_sem=recv,
            device_id=(fs_to, tp_to), device_id_type=MESH,
        )

    def columns(owner):
        return pl.ds(pl.multiple_of(owner * col, col), col)

    def slab(v):
        return v // cuts, pl.ds(pl.multiple_of(v % cuts * block, block), block)

    def only(condition, needed, action):
        if needed:
            pl.when(condition)(action)
        else:
            action()

    lead = [(a, v) for v in range(special) for a in range(2)]
    early, late = lead[:special], lead[special:]
    split, final = (0, blocks - 1), (1, blocks - 1)
    lead.append(split)
    middle = [(a, v) for v in range(special, blocks - 1) for a in range(2)]
    pieces = lead + middle + [final]
    ahead = list(range(special // cuts))
    after = {}
    for e in range(experts):
        inside = [n for n, (a, v) in enumerate(pieces[:-1]) if v // cuts == e and (a, v) in middle]
        after.setdefault(inside[-1] if inside else len(pieces) - 1, []).append(e)
    for e in ahead:
        after = {n: [i for i in held if i != e] for n, held in after.items()}
        after.setdefault(2 * cuts * (e + 1) - 1, []).append(e)
    kept = pl.ds(depth // 2, depth // 2)

    def crossing(a, v):
        return remote(
            own.at[a, v], far.at[side, a, v], across_send.at[a, v], across_recv.at[side, a, v],
            fs, beyond + relay_side,
        )

    def crossing_part(a, v):
        return remote(
            own.at[a, v, kept], far.at[side, a, v, kept], across_send.at[a, v],
            across_recv.at[side, a, v], fs, beyond + relay_side,
        )

    def deal(source, a, v, owner, sem, low=0):
        e, at = slab(v)
        rows = pl.ds(pl.multiple_of(fs * depth + low, depth - low), depth - low)
        for h in range(per):
            remote(
                source.at[:, pl.ds(h * block, block)],
                full[a].at[e, rows, at],
                sem,
                near_recv.at[a, v],
                owner * per + h,
                half * 2 + 1 - owner % 2,
            ).start()

    def fetch(n):
        a, v = pieces[n]
        for h in range(per):
            pltpu.make_async_copy(
                (gate_f32, up_f32)[a].at[
                    v // cuts, :, pl.ds(h * units + v % cuts * block, block)
                ],
                stage.at[n % 2, :, pl.ds(h * block, block)],
                load.at[n % 2],
            ).start()

    def fetched(n):
        pltpu.make_async_copy(stage.at[n % 2], stage.at[n % 2], load.at[n % 2]).wait()

    def fetch_down(e):
        return pltpu.make_async_copy(down_f32.at[e], down_stage.at[e % 2], load.at[2 + e % 2])

    def down_local(e):
        return pltpu.make_async_copy(
            down.at[e], down_all.at[e, :, columns(tp)], local_sem.at[4 + e]
        )

    def down_to(k, e):
        return remote(
            down.at[e], down_all.at[e, :, columns(tp)], down_send.at[k, e],
            down_recv.at[(0, 1 + side)[k], e], fs, (twin, beyond + relay_side)[k],
        )

    def down_pass(s, e):
        part = down_all.at[e, :, columns(beyond + s)]
        return remote(part, part, down_send.at[2 + s, e], down_recv.at[1 + s, e], fs, twin)

    tile = min(depth, 32)
    fetch(0)
    token_copy = pltpu.make_async_copy(tokens, x, local_sem.at[0])
    token_copy.start()
    spot = lax.broadcasted_iota(jnp.int32, (depth, depth), 0)
    lane = lax.broadcasted_iota(jnp.int32, (depth, depth), 1)
    factor = jnp.sum(jnp.where(spot == lane, gain[...], 0.0), axis=1, keepdims=True)
    weight[0:depth, :] = jnp.broadcast_to(factor, (depth, weight.shape[1]))
    for n, piece in enumerate(pieces):
        a, v = piece
        if n + 1 < len(pieces):
            fetch(n + 1)
        if n == 0:
            fetch_down(0).start()
            fetch_down(1).start()
        fetched(n)

        def scale(i, carry, a=a, v=v, n=n):
            at = pl.ds(pl.multiple_of(i * tile, tile), tile)
            own[a, v, at, :] = (stage[n % 2, at, :] * weight[at, 0:1]).astype(own.dtype)
            return carry

        lax.fori_loop(0, depth // tile, scale, 0)
        only(close, piece in late or piece == split, lambda: crossing(a, v).start())
        if piece == split:
            pl.when(apart)(lambda: crossing_part(a, v).start())
        only(close, piece in early, lambda: deal(own.at[a, v], a, v, tp, near_send.at[a, v]))
        for e in after.get(n, []):
            fetch_down(e).wait()
            short = min(units, 128)

            def narrow(i, carry, e=e):
                at = pl.ds(pl.multiple_of(i * short, short), short)
                down[e, at, :] = down_stage[e % 2, at, :].astype(down.dtype)
                return carry

            lax.fori_loop(0, units // short, narrow, 0)
            if e + 2 < experts:
                fetch_down(e + 2).start()
            down_to(1, e).start()
            down_to(0, e).start()
            down_local(e).start()

    token_copy.wait()
    count = x.shape[0]
    strip = count // 8

    def normalise(i, carry):
        at = pl.ds(pl.multiple_of(i * strip, strip), strip)
        floats = x[at, :].astype(jnp.float32)
        x[at, :] = (
            floats * lax.rsqrt(jnp.mean(floats * floats, axis=1, keepdims=True) + EPS)
        ).astype(x.dtype)
        return carry

    lax.fori_loop(0, count // strip, normalise, 0)
    first = jax.nn.sigmoid(logit[0:1, :] - logit[1:2, :])
    expert_of = lax.broadcasted_iota(jnp.int32, (weight.shape[1], count), 0)
    by_expert = jnp.where(routes[0:1, :] == expert_of, first, 0.0) + jnp.where(
        routes[1:2, :] == expert_of, 1.0 - first, 0.0
    )
    weight[...] = by_expert.T
    total[...] = jnp.zeros_like(total)

    def relay(a, v, low=0):
        for s in range(2):
            part = far.at[s, a, v, pl.ds(low, depth - low)]
            pltpu.make_async_copy(part, part, across_recv.at[s, a, v]).wait()
            deal(part, a, v, beyond + s, far_send.at[s, a, v], low)

    def relay_down(e):
        for s in range(2):
            down_pass(s, e).wait_recv()
            down_pass(s, e).start()

    away = pl.ds(pl.multiple_of((1 - group // 2) * (features // 2), features // 2), features // 2)

    def hand(a, v):
        e, at = slab(v)
        part = full[a].at[e, :, at]
        return remote(part, part, twin_send.at[a, v], twin_recv.at[a, v], fs, twin)

    sources = features // depth // 2

    def onward(a, v):
        e, at = slab(v)
        if (a, v) != split:
            part = full[a].at[e, away, at]
            remote(
                part, part, onward_send.at[a, v], near_recv.at[a, v], fs, beyond + side
            ).start()
        else:

            def send(i, carry):
                start = ((1 - group // 2) * sources + i) * depth
                part = full[a].at[e, pl.ds(pl.multiple_of(start, depth), depth // 2), at]
                remote(
                    part, part, onward_send.at[a, v], near_recv.at[a, v], fs, beyond + side
                ).start()
                return carry

            lax.fori_loop(0, sources, send, 0)

    def onward_sent(a, v):
        e, at = slab(v)
        count = features // (4 if (a, v) == split else 2)
        part = full[a].at[e, pl.ds(0, count), at]
        pltpu.make_async_copy(part, part, onward_send.at[a, v]).wait()

    def take(a, v, forward):
        e, at = slab(v)
        part = full[a].at[e, :, at]
        pltpu.make_async_copy(part, part, near_recv.at[a, v]).wait()
        if forward:
            onward(a, v)
        hand(a, v).start()

    def take_all(group_of, forward):
        for a, v in group_of:
            take(a, v, forward)

    @pl.when(jnp.logical_not(lands))
    def _():
        for n, (a, v) in enumerate(lead):
            only(apart, (a, v) in late or (a, v) == split, functools.partial(relay, a, v))
            if (a, v) == split:
                pl.when(close)(functools.partial(relay, a, v, depth // 2))
            for e in after.get(n, []):
                relay_down(e)

        def pass_on(v, carry):
            relay(0, v)
            relay(1, v)
            last = jnp.logical_or(v % cuts == cuts - 1, v == blocks - 2)
            pl.when(last)(lambda: relay_down(v // cuts))
            return carry

        lax.fori_loop(special, blocks - 1, pass_on, 0)
        relay(*final)
        for e in after.get(len(pieces) - 1, []):
            relay_down(e)

    moved = late + [split]

    @pl.when(lands)
    def _():
        pl.when(close)(lambda: take_all(moved, True))
        pl.when(apart)(lambda: take_all(early, True))

    def arrive(v):
        @pl.when(lands)
        def _():
            take(0, v, False)
            take(1, v, False)

        @pl.when(jnp.logical_not(lands))
        def _():
            hand(0, v).wait_recv()
            hand(1, v).wait_recv()

    def down_ready(e):
        down_local(e).wait()
        down_to(0, e).wait_recv()

        @pl.when(lands)
        def _():
            for s in range(2):
                down_pass(s, e).wait_recv()

    def bring(a, v, i):
        e, at = slab(v)
        return pltpu.make_async_copy(full[a].at[e, :, at], wide.at[i, a], fetch_sem.at[3 * i + a])

    def bring_down(v, i):
        e, at = slab(v)
        return pltpu.make_async_copy(down_all.at[e, at, :], tall.at[i], fetch_sem.at[3 * i + 2])

    def compute(v):
        e, at = slab(v)
        copies = [bring(0, v, 0), bring(1, v, 0), bring_down(v, 0)]
        for copy in copies:
            copy.start()
        for copy in copies:
            copy.wait()
        expert_rows(x, weight, wide.at[0], tall.at[0], total, e)

    for e in range(special // cuts):
        down_ready(e)

    def turn(v, carry):
        arrive(v)
        pl.when(jnp.logical_or(v % cuts == 0, v == special))(lambda: down_ready(v // cuts))
        compute(v)
        return carry

    lax.fori_loop(special, blocks - 1, turn, 0)

    @pl.when(jnp.logical_and(lands, close))
    def _():
        take_all(early, False)

    for v in range(special // 2):

        @pl.when(jnp.logical_not(lands))
        def _(v=v):
            hand(0, v).wait_recv()
            hand(1, v).wait_recv()

        compute(v)
    if (blocks - 1) // cuts != (blocks - 2) // cuts:
        down_ready(experts - 1)
    ends = list(range(special // 2, special)) + [blocks - 1]
    for i, v in enumerate(ends):
        bring_down(v, i).start()
    coming = [p for p in lead[special // 2 * 2 :] + [final]]

    @pl.when(jnp.logical_and(lands, apart))
    def _():
        take_all(moved, False)

    @pl.when(lands)
    def _():
        take_all([final], False)

    @pl.when(jnp.logical_not(lands))
    def _():
        for a, v in coming:
            hand(a, v).wait_recv()

    for a, v in coming:
        bring(a, v, ends.index(v)).start()
    for i, v in enumerate(ends):
        bring_down(v, i).wait()
        bring(0, v, i).wait()
        bring(1, v, i).wait()

    highs, _, owned, width = part.shape
    high, low = fs // 2, fs % 2
    tiles = min(highs, 4)
    held = highs // tiles
    span = count // tiles
    column = width // 2

    def tile_of(k):
        return lax.rem(high // held + k, tiles)

    def low_copy(k, c):
        t = tile_of(k)
        at, over = pl.ds(t * held, held), pl.ds(c * column, column)
        return remote(
            part.at[at, 1 - low, :, over], low_in.at[at, :, over],
            low_send.at[t, c], low_recv.at[t, c], high * 2 + 1 - low, tp,
        )

    def high_copy(shift, c):
        to = lax.rem(high + shift, highs)
        over = pl.ds(c * column, column)
        return remote(
            mid.at[to, :, over], high_in.at[shift, :, over],
            high_send.at[shift, c], high_recv.at[shift, c], to * 2 + low, tp,
        )

    def merge(k):
        t = tile_of(k)
        for c in range(2):
            over = pl.ds(c * column, column)
            low_copy(k, c).wait_recv()
            for n in range(held):
                to = t * held + n
                mid[to, :, over] = (
                    part[to, low, :, over].astype(jnp.float32)
                    + low_in[to, :, over].astype(jnp.float32)
                ).astype(mid.dtype)

                @pl.when(to != high)
                def _(to=to):
                    high_copy(lax.rem(to - high + highs, highs), c).start()

    def closing(k, carry):
        t = tile_of(k)
        at = pl.ds(pl.multiple_of(t * span, span), span)
        for i, v in enumerate(ends):
            expert_tile(x, weight, wide.at[i], tall.at[i], total, v // cuts, at)
        values = total[at, :]
        for n in range(held):
            for side_of in range(2):
                start = (n * 2 + side_of) * owned
                part[t * held + n, side_of] = values[start : start + owned].astype(part.dtype)
        for c in range(2):
            low_copy(k, c).start()
        pl.when(k >= 2)(lambda: merge(k - 1))
        return carry

    lax.fori_loop(1, tiles + 1, closing, 0)
    merge(tiles)
    for c in range(2):
        over = pl.ds(c * column, column)
        gathered = part[high, low, :, over].astype(jnp.float32) + low_in[high, :, over].astype(
            jnp.float32
        )
        for shift in range(1, highs):
            high_copy(shift, c).wait_recv()
            gathered = gathered + high_in[shift, :, over].astype(jnp.float32)
        mixed[:, over] = gathered.astype(mixed.dtype)
    for c in range(2):
        for k in range(tiles):
            low_copy(k, c).wait_send()
        for shift in range(1, highs):
            high_copy(shift, c).wait_send()

    @pl.when(lands)
    def _():
        for a, v in pieces:
            hand(a, v).wait_send()

        def sent(group_of):
            for a, v in group_of:
                onward_sent(a, v)

        pl.when(close)(lambda: sent(moved))
        pl.when(apart)(lambda: sent(early))

    @pl.when(jnp.logical_not(lands))
    def _():
        for s in range(2):
            for a, v in pieces:

                def gone(low, s=s, a=a, v=v):
                    part = far.at[s, a, v, pl.ds(low, depth - low)]
                    pltpu.make_async_copy(part, part, far_send.at[s, a, v]).wait()

                only(apart, (a, v) in moved, functools.partial(gone, 0))
                if (a, v) == split:
                    pl.when(close)(functools.partial(gone, depth // 2))
            for e in range(experts):
                down_pass(s, e).wait_send()

    for piece in pieces:
        a, v = piece

        def dealt(sem, a=a, v=v):
            pltpu.make_async_copy(own.at[a, v], own.at[a, v], sem).wait()

        only(close, piece in moved, lambda: crossing(a, v).wait_send())
        if piece == split:
            pl.when(apart)(lambda: crossing_part(a, v).wait_send())
        only(close, piece in early, lambda: dealt(near_send.at[a, v]))
    for e in range(experts):
        down_to(0, e).wait_send()
        down_to(1, e).wait_send()


def finish(gate_in, up_in, down_in, mixed_in, gate, up, down, mixed, ring, small, take, put, side):
    slots, rows, width = ring.shape
    steps = []
    for source, target in ((gate_in, gate), (up_in, up), (down_in, down)):
        experts, height, span = source.shape
        for e in range(experts):
            for r in range(0, height, min(height, rows)):
                for c in range(0, span, width):
                    at = (e, pl.ds(r, min(height, rows)), pl.ds(c, width))
                    steps.append((source.at[at], target.at[at], min(height, rows)))

    def pull(n):
        source, _, height = steps[n]
        slot = n % slots
        return pltpu.make_async_copy(source, ring.at[slot, pl.ds(0, height)], take.at[slot])

    def push(n):
        _, target, height = steps[n]
        slot = n % slots
        return pltpu.make_async_copy(ring.at[slot, pl.ds(0, height)], target, put.at[slot])

    ahead = slots // 2
    inward = pltpu.make_async_copy(mixed_in, small, side.at[0])
    inward.start()
    for n in range(min(ahead, len(steps))):
        pull(n).start()
    for n in range(len(steps)):
        if n + ahead < len(steps):
            if n + ahead >= slots:
                push(n + ahead - slots).wait()
            pull(n + ahead).start()
        pull(n).wait()
        push(n).start()
    inward.wait()
    outward = pltpu.make_async_copy(small, mixed, side.at[1])
    outward.start()
    for n in range(max(0, len(steps) - slots), len(steps)):
        push(n).wait()
    outward.wait()


def shards(fs_size, tokens, norm_gain, gate_weight, up_weight, down_weight, routes, route_logit):
    experts, depth, width = gate_weight.shape
    _, units, col = down_weight.shape
    rows, features = tokens.shape
    half = jnp.bfloat16
    anywhere = pl.BlockSpec(memory_space=pl.ANY)
    vmem = pl.BlockSpec(memory_space=pltpu.VMEM)
    dma = pltpu.SemaphoreType.DMA
    block = min(units, 512)
    cuts = units // block
    blocks = experts * cuts
    special = blocks // 2 - 1
    both = width // cuts
    gate_shape = jax.ShapeDtypeStruct((experts, features, units), half)
    down_shape = jax.ShapeDtypeStruct((experts, units, features), half)
    highs, owned = fs_size // 2, rows // fs_size
    tiles = min(highs, 4)
    last = special - special // 2 + 1
    mixed_shape = jax.ShapeDtypeStruct((owned, features), half)
    gate_all, up_all, down_all, _, summed = pl.pallas_call(
        functools.partial(spread, cuts, special),
        out_shape=(
            gate_shape, gate_shape, down_shape,
            jax.ShapeDtypeStruct((2, 2, blocks, depth, both), half),
            mixed_shape,
        ),
        in_specs=[vmem, anywhere, vmem, vmem] + [anywhere] * 3,
        out_specs=(anywhere,) * 4 + (vmem,),
        scratch_shapes=[
            pltpu.VMEM((2, blocks, depth, both), half),
            pltpu.VMEM((experts, units, col), half),
            pltpu.VMEM((2, depth, both), jnp.float32),
            pltpu.VMEM((2, units, col), jnp.float32),
            pltpu.VMEM((rows, features), half),
            pltpu.VMEM((rows, 128), jnp.float32),
            pltpu.VMEM((rows, features), jnp.float32),
            pltpu.VMEM((last, 2, features, block), half),
            pltpu.VMEM((last, block, features), half),
            pltpu.VMEM((highs, 2, owned, features), half),
            pltpu.VMEM((highs, owned, features), half),
            pltpu.VMEM((highs, owned, features), half),
            pltpu.VMEM((highs, owned, features), half),
            dma((4,)),
        ]
        + [dma((2, blocks)), dma((2, 2, blocks))]
        + [dma((2, blocks))] * 2
        + [dma((2, 2, blocks))]
        + [dma((2, blocks))] * 3
        + [dma((4, experts)), dma((3, experts))]
        + [dma((4 + experts,)), dma((3 * last,))]
        + [dma((tiles, 2))] * 2
        + [dma((highs, 2))] * 2,
        compiler_params=pltpu.CompilerParams(
            has_side_effects=True, vmem_limit_bytes=VMEM_LIMIT
        ),
        name="spread",
    )(norm_gain[None, :], tokens, routes.T, route_logit.T, gate_weight, up_weight, down_weight)

    slots = 8
    gate_out, up_out, down_out, mixed = pl.pallas_call(
        finish,
        out_shape=(gate_shape, gate_shape, down_shape, mixed_shape),
        in_specs=[anywhere] * 4,
        out_specs=(anywhere,) * 4,
        scratch_shapes=[
            pltpu.VMEM((slots, features, units), half),
            pltpu.VMEM((owned, features), half),
            dma((slots,)), dma((slots,)), dma((2,)),
        ],
        compiler_params=pltpu.CompilerParams(vmem_limit_bytes=VMEM_LIMIT),
        name="finish",
    )(gate_all, up_all, down_all, summed)
    return (gate_out, up_out, down_out, mixed)


def solution(mesh):
    return jax.shard_map(
        functools.partial(shards, mesh.shape["fs"]),
        mesh=mesh,
        in_specs=(
            P("tp", None),
            P("fs"),
            P(None, "fs", "tp"),
            P(None, "fs", "tp"),
            P(None, "fs", "tp"),
            P("tp", None),
            P("tp", None),
        ),
        out_specs=(
            P(None, None, "fs"),
            P(None, None, "fs"),
            P(None, "fs", None),
            P(("tp", "fs"), None),
        ),
        check_vma=False,
    )
```

```python
import functools

import jax
import jax.numpy as jnp
from jax import lax
from jax.experimental import pallas as pl
from jax.experimental.pallas import tpu as pltpu
from jax.sharding import PartitionSpec as P

EPS = 0.5
QUARTERS = 1
MESH = pl.DeviceIdType.MESH
VMEM_LIMIT = 63 * 1024 * 1024


def expert_tile(x, weight, wide, tall, total, expert, at):
    mine = x[at, :]
    gate_val = jnp.dot(mine, wide[0], preferred_element_type=jnp.float32)
    up_val = jnp.dot(mine, wide[1], preferred_element_type=jnp.float32)
    hidden = (jax.nn.silu(gate_val) * up_val).astype(jnp.bfloat16)
    result = jnp.dot(hidden, tall[...], preferred_element_type=jnp.float32)
    shares = weight[at, :]
    lane = lax.broadcasted_iota(jnp.int32, shares.shape, 1)
    share = jnp.sum(jnp.where(lane == expert, shares, 0.0), axis=1, keepdims=True)
    total[at, :] += share * result


def expert_rows(x, weight, wide, tall, total, expert):
    rows = x.shape[0]
    tile = rows // 2

    def step(i, carry):
        at = pl.ds(pl.multiple_of(i * tile, tile), tile)
        expert_tile(x, weight, wide, tall, total, expert, at)
        return carry

    lax.fori_loop(0, rows // tile, step, 0)


def spread(
    cuts, special, fs_size, tp_size,
    gain, tokens, routes, logit, gate_f32, up_f32, down_f32,
    gate_all, up_all, down_all, far, mixed,
    own, down, stage, down_stage, x, weight, total, wide, tall, part, low_in, mid, high_in,
    load, across_send, across_recv, near_send, near_recv, far_send, twin_send, twin_recv,
    onward_send, down_send, down_recv, local_sem, fetch_sem,
    low_send, low_recv, high_send, high_recv,
):
    _, blocks, depth, both = own.shape
    experts = blocks // cuts
    features, units = gate_all.shape[1:]
    block = units // cuts
    per = both // block
    fs, tp = lax.axis_index("fs"), lax.axis_index("tp")
    half, side = tp // 2, tp % 2
    twin = half * 2 + 1 - side
    col = down.shape[2]
    group = fs // per
    relay_side = group % 2
    lands = side != relay_side
    beyond = (1 - half) * 2
    apart = group // 2 != half
    close = group // 2 == half
    full = (gate_all, up_all)

    def remote(src, dst, send, recv, fs_to, tp_to):
        return pltpu.make_async_remote_copy(
            src_ref=src, dst_ref=dst, send_sem=send, recv_sem=recv,
            device_id=(fs_to, tp_to), device_id_type=MESH,
        )

    def columns(owner):
        return pl.ds(pl.multiple_of(owner * col, col), col)

    def slab(v):
        return v // cuts, pl.ds(pl.multiple_of(v % cuts * block, block), block)

    def only(condition, needed, action):
        if needed:
            pl.when(condition)(action)
        else:
            action()

    lead = [(a, v) for v in range(special) for a in range(2)]
    early, late = lead[:special], lead[special:]
    split, final = (0, blocks - 1), (1, blocks - 1)
    lead.append(split)
    middle = [(a, v) for v in range(special, blocks - 1) for a in range(2)]
    pieces = lead + middle + [final]
    ahead = list(range(special // cuts))
    after = {}
    for e in range(experts):
        inside = [n for n, (a, v) in enumerate(pieces[:-1]) if v // cuts == e and (a, v) in middle]
        after.setdefault(inside[-1] if inside else len(pieces) - 1, []).append(e)
    for e in ahead:
        after = {n: [i for i in held if i != e] for n, held in after.items()}
        after.setdefault(2 * cuts * (e + 1) - 1, []).append(e)
    moving = depth * QUARTERS // 4
    kept = pl.ds(moving, depth - moving)

    def crossing(a, v):
        return remote(
            own.at[a, v], far.at[side, a, v], across_send.at[a, v], across_recv.at[side, a, v],
            fs, beyond + relay_side,
        )

    def crossing_part(a, v):
        return remote(
            own.at[a, v, kept], far.at[side, a, v, kept], across_send.at[a, v],
            across_recv.at[side, a, v], fs, beyond + relay_side,
        )

    def deal(source, a, v, owner, sem, low=0):
        e, at = slab(v)
        rows = pl.ds(pl.multiple_of(fs * depth + low, low or depth), depth - low)
        for h in range(per):
            remote(
                source.at[:, pl.ds(h * block, block)],
                full[a].at[e, rows, at],
                sem,
                near_recv.at[a, v],
                owner * per + h,
                half * 2 + 1 - owner % 2,
            ).start()

    def fetch(n):
        a, v = pieces[n]
        for h in range(per):
            pltpu.make_async_copy(
                (gate_f32, up_f32)[a].at[
                    v // cuts, :, pl.ds(h * units + v % cuts * block, block)
                ],
                stage.at[n % 2, :, pl.ds(h * block, block)],
                load.at[n % 2],
            ).start()

    def fetched(n):
        pltpu.make_async_copy(stage.at[n % 2], stage.at[n % 2], load.at[n % 2]).wait()

    def fetch_down(e):
        return pltpu.make_async_copy(down_f32.at[e], down_stage.at[e % 2], load.at[2 + e % 2])

    def down_local(e):
        return pltpu.make_async_copy(
            down.at[e], down_all.at[e, :, columns(tp)], local_sem.at[4 + e]
        )

    def down_to(k, e):
        return remote(
            down.at[e], down_all.at[e, :, columns(tp)], down_send.at[k, e],
            down_recv.at[(0, 1 + side)[k], e], fs, (twin, beyond + relay_side)[k],
        )

    def down_pass(s, e):
        part = down_all.at[e, :, columns(beyond + s)]
        return remote(part, part, down_send.at[2 + s, e], down_recv.at[1 + s, e], fs, twin)

    def relay(a, v, low=0):
        for s in range(2):
            part = far.at[s, a, v, pl.ds(low, depth - low)]
            pltpu.make_async_copy(part, part, across_recv.at[s, a, v]).wait()
            deal(part, a, v, beyond + s, far_send.at[s, a, v], low)

    met = pltpu.get_barrier_semaphore()

    def greet():
        def signal(i, carry):
            to = lax.rem(fs * tp_size + tp + i, fs_size * tp_size)
            pl.semaphore_signal(
                met, inc=1, device_id=(to // tp_size, to % tp_size), device_id_type=MESH
            )
            return carry

        lax.fori_loop(1, fs_size * tp_size, signal, 0)

    def meet():
        pl.semaphore_wait(met, fs_size * tp_size - 1)

    turns = {len(pieces) // 2 + 3 * i: piece for i, piece in enumerate(early)}

    tile = min(depth, 32)
    greet()
    fetch(0)
    token_copy = pltpu.make_async_copy(tokens, x, local_sem.at[0])
    token_copy.start()
    spot = lax.broadcasted_iota(jnp.int32, (depth, depth), 0)
    lane = lax.broadcasted_iota(jnp.int32, (depth, depth), 1)
    factor = jnp.sum(jnp.where(spot == lane, gain[...], 0.0), axis=1, keepdims=True)
    weight[0:depth, :] = jnp.broadcast_to(factor, (depth, weight.shape[1]))
    for n, piece in enumerate(pieces):
        a, v = piece
        if n + 1 < len(pieces):
            fetch(n + 1)
        if n == 0:
            fetch_down(0).start()
            fetch_down(1).start()
        fetched(n)
        if n == 0:
            meet()

        def scale(i, carry, a=a, v=v, n=n):
            at = pl.ds(pl.multiple_of(i * tile, tile), tile)
            own[a, v, at, :] = (stage[n % 2, at, :] * weight[at, 0:1]).astype(own.dtype)
            return carry

        lax.fori_loop(0, depth // tile, scale, 0)
        only(close, piece in late or piece == split, lambda: crossing(a, v).start())
        if piece == split:
            pl.when(apart)(lambda: crossing_part(a, v).start())
        only(close, piece in early, lambda: deal(own.at[a, v], a, v, tp, near_send.at[a, v]))
        for e in after.get(n, []):
            fetch_down(e).wait()
            short = min(units, 128)

            def narrow(i, carry, e=e):
                at = pl.ds(pl.multiple_of(i * short, short), short)
                down[e, at, :] = down_stage[e % 2, at, :].astype(down.dtype)
                return carry

            lax.fori_loop(0, units // short, narrow, 0)
            if e + 2 < experts:
                fetch_down(e + 2).start()
            down_to(1, e).start()
            down_to(0, e).start()
            down_local(e).start()
        if n in turns:
            pl.when(jnp.logical_not(lands))(functools.partial(relay, *turns[n]))
    for n, piece in turns.items():
        if n >= len(pieces):
            pl.when(jnp.logical_not(lands))(functools.partial(relay, *piece))

    token_copy.wait()
    count = x.shape[0]
    strip = count // 8

    def normalise(i, carry):
        at = pl.ds(pl.multiple_of(i * strip, strip), strip)
        floats = x[at, :].astype(jnp.float32)
        x[at, :] = (
            floats * lax.rsqrt(jnp.mean(floats * floats, axis=1, keepdims=True) + EPS)
        ).astype(x.dtype)
        return carry

    lax.fori_loop(0, count // strip, normalise, 0)
    first = jax.nn.sigmoid(logit[0:1, :] - logit[1:2, :])
    expert_of = lax.broadcasted_iota(jnp.int32, (weight.shape[1], count), 0)
    by_expert = jnp.where(routes[0:1, :] == expert_of, first, 0.0) + jnp.where(
        routes[1:2, :] == expert_of, 1.0 - first, 0.0
    )
    weight[...] = by_expert.T
    total[...] = jnp.zeros_like(total)

    def relay_down(e):
        for s in range(2):
            down_pass(s, e).wait_recv()
            down_pass(s, e).start()

    away = pl.ds(pl.multiple_of((1 - group // 2) * (features // 2), features // 2), features // 2)

    def hand(a, v):
        e, at = slab(v)
        part = full[a].at[e, :, at]
        return remote(part, part, twin_send.at[a, v], twin_recv.at[a, v], fs, twin)

    sources = features // depth // 2

    def onward(a, v):
        e, at = slab(v)
        if (a, v) != split:
            part = full[a].at[e, away, at]
            remote(
                part, part, onward_send.at[a, v], near_recv.at[a, v], fs, beyond + side
            ).start()
        else:

            def send(i, carry):
                start = ((1 - group // 2) * sources + i) * depth
                part = full[a].at[e, pl.ds(pl.multiple_of(start, depth), moving), at]
                remote(
                    part, part, onward_send.at[a, v], near_recv.at[a, v], fs, beyond + side
                ).start()
                return carry

            lax.fori_loop(0, sources, send, 0)

    def onward_sent(a, v):
        e, at = slab(v)
        count = sources * (moving if (a, v) == split else depth)
        part = full[a].at[e, pl.ds(0, count), at]
        pltpu.make_async_copy(part, part, onward_send.at[a, v]).wait()

    def take(a, v, forward):
        e, at = slab(v)
        part = full[a].at[e, :, at]
        pltpu.make_async_copy(part, part, near_recv.at[a, v]).wait()
        if forward:
            onward(a, v)
        hand(a, v).start()

    def take_all(group_of, forward):
        for a, v in group_of:
            take(a, v, forward)

    @pl.when(jnp.logical_not(lands))
    def _():
        for n, (a, v) in enumerate(lead):
            if (a, v) not in early:
                pl.when(apart)(functools.partial(relay, a, v))
            if (a, v) == split:
                pl.when(close)(functools.partial(relay, a, v, moving))
            for e in after.get(n, []):
                relay_down(e)

    moved = late + [split]

    @pl.when(lands)
    def _():
        pl.when(close)(lambda: take_all(moved, True))
        pl.when(apart)(lambda: take_all(early, True))

    def arrive(v):
        @pl.when(lands)
        def _():
            take(0, v, False)
            take(1, v, False)

        @pl.when(jnp.logical_not(lands))
        def _():
            hand(0, v).wait_recv()
            hand(1, v).wait_recv()

    def down_ready(e):
        down_local(e).wait()
        down_to(0, e).wait_recv()

        @pl.when(lands)
        def _():
            for s in range(2):
                down_pass(s, e).wait_recv()

    def bring(a, v, i):
        e, at = slab(v)
        return pltpu.make_async_copy(full[a].at[e, :, at], wide.at[i, a], fetch_sem.at[3 * i + a])

    def bring_down(v, i):
        e, at = slab(v)
        return pltpu.make_async_copy(down_all.at[e, at, :], tall.at[i], fetch_sem.at[3 * i + 2])

    def compute(v):
        e, at = slab(v)
        copies = [bring(0, v, 0), bring(1, v, 0), bring_down(v, 0)]
        for copy in copies:
            copy.start()
        for copy in copies:
            copy.wait()
        expert_rows(x, weight, wide.at[0], tall.at[0], total, e)

    for e in range(special // cuts):
        down_ready(e)

    def pass_on(v):
        @pl.when(v < blocks - 1)
        def _():
            relay(0, v)
            relay(1, v)
            last = jnp.logical_or(v % cuts == cuts - 1, v == blocks - 2)
            pl.when(last)(lambda: relay_down(v // cuts))

        @pl.when(v == blocks - 1)
        def _():
            relay(*final)
            for e in after.get(len(pieces) - 1, []):
                relay_down(e)

    def turn(v, carry):
        pl.when(jnp.logical_not(lands))(lambda: pass_on(v))

        @pl.when(v >= special + lag)
        def _():
            w = v - lag
            arrive(w)
            pl.when(jnp.logical_or(w % cuts == 0, w == special))(lambda: down_ready(w // cuts))
            compute(w)

        return carry

    lag = 2
    lax.fori_loop(special, blocks, turn, 0)

    @pl.when(jnp.logical_and(lands, close))
    def _():
        take_all(early, False)

    for v in range(special // 2):

        @pl.when(jnp.logical_not(lands))
        def _(v=v):
            hand(0, v).wait_recv()
            hand(1, v).wait_recv()

        compute(v)
    arrive(blocks - 2)
    if (blocks - 2) % cuts == 0 or blocks - 2 == special:
        down_ready((blocks - 2) // cuts)
    compute(blocks - 2)
    if (blocks - 1) // cuts != (blocks - 2) // cuts:
        down_ready(experts - 1)
    ends = list(range(special // 2, special)) + [blocks - 1]
    for i, v in enumerate(ends):
        bring_down(v, i).start()
    coming = [p for p in lead[special // 2 * 2 :] + [final]]

    @pl.when(jnp.logical_and(lands, apart))
    def _():
        take_all(moved, False)

    @pl.when(lands)
    def _():
        take_all([final], False)

    @pl.when(jnp.logical_not(lands))
    def _():
        for a, v in coming:
            hand(a, v).wait_recv()

    for a, v in coming:
        bring(a, v, ends.index(v)).start()
    for i, v in enumerate(ends):
        bring_down(v, i).wait()
        bring(0, v, i).wait()
        bring(1, v, i).wait()

    highs, _, owned, width = part.shape
    high, low = fs // 2, fs % 2
    tiles = min(highs, 4)
    held = highs // tiles
    span = count // tiles
    column = width // 2

    paired = held == 1 and tiles == 4

    def flip(value, mask):
        ones, twos = value % 2, value // 2
        low_bit = ones + mask % 2 - 2 * ones * (mask % 2)
        return low_bit + 2 * (twos + mask // 2 - 2 * twos * (mask // 2))

    def tile_of(k):
        return flip(high, tiles - k) if paired else lax.rem(high // held + k, tiles)

    def low_copy(k, c):
        t = tile_of(k)
        at, over = pl.ds(t * held, held), pl.ds(c * column, column)
        return remote(
            part.at[at, 1 - low, :, over], low_in.at[at, :, over],
            low_send.at[t, c], low_recv.at[t, c], high * 2 + 1 - low, tp,
        )

    def high_copy(shift, c):
        to = lax.rem(high + shift, highs)
        over = pl.ds(c * column, column)
        return remote(
            mid.at[to, :, over], high_in.at[shift, :, over],
            high_send.at[shift, c], high_recv.at[shift, c], to * 2 + low, tp,
        )

    def pair_copy(k, c):
        over = pl.ds(c * column, column)
        to = flip(high, 2 if k == 2 else 1)
        return remote(
            mid.at[tile_of(k), :, over], high_in.at[k, :, over],
            high_send.at[k, c], high_recv.at[k, c], to * 2 + low, tp,
        )

    def pair_merge(k):
        t = tile_of(k)
        for c in range(2):
            over = pl.ds(c * column, column)
            low_copy(k, c).wait_recv()
            sums = part[t, low, :, over].astype(jnp.float32) + low_in[t, :, over].astype(
                jnp.float32
            )
            if k == 2:
                pair_copy(1, c).wait_recv()
                sums = sums + high_in[1, :, over].astype(jnp.float32)
            mid[t, :, over] = sums.astype(mid.dtype)
            pair_copy(k, c).start()

    def merge(k):
        t = tile_of(k)
        for c in range(2):
            over = pl.ds(c * column, column)
            low_copy(k, c).wait_recv()
            for n in range(held):
                to = t * held + n
                mid[to, :, over] = (
                    part[to, low, :, over].astype(jnp.float32)
                    + low_in[to, :, over].astype(jnp.float32)
                ).astype(mid.dtype)

                @pl.when(to != high)
                def _(to=to):
                    high_copy(lax.rem(to - high + highs, highs), c).start()

    def closing(k, carry):
        t = tile_of(k)
        at = pl.ds(pl.multiple_of(t * span, span), span)
        for i, v in enumerate(ends):
            expert_tile(x, weight, wide.at[i], tall.at[i], total, v // cuts, at)
        values = total[at, :]
        for n in range(held):
            for side_of in range(2):
                start = (n * 2 + side_of) * owned
                part[t * held + n, side_of] = values[start : start + owned].astype(part.dtype)
        for c in range(2):
            low_copy(k, c).start()
        if paired:
            for step in range(1, tiles):
                pl.when(k == step + 1)(functools.partial(pair_merge, step))
        else:
            pl.when(k >= 2)(lambda: merge(k - 1))
        return carry

    lax.fori_loop(1, tiles + 1, closing, 0)
    if not paired:
        merge(tiles)
    for c in range(2):
        over = pl.ds(c * column, column)
        if paired:
            low_copy(tiles, c).wait_recv()
        gathered = part[high, low, :, over].astype(jnp.float32) + low_in[high, :, over].astype(
            jnp.float32
        )
        for shift in (2, 3) if paired else range(1, highs):
            (pair_copy if paired else high_copy)(shift, c).wait_recv()
            gathered = gathered + high_in[shift, :, over].astype(jnp.float32)
        mixed[:, over] = gathered.astype(mixed.dtype)
    for c in range(2):
        for k in range(1, tiles + 1):
            low_copy(k, c).wait_send()
        for shift in range(1, highs):
            (pair_copy if paired else high_copy)(shift, c).wait_send()

    @pl.when(lands)
    def _():
        for a, v in pieces:
            hand(a, v).wait_send()

        def sent(group_of):
            for a, v in group_of:
                onward_sent(a, v)

        pl.when(close)(lambda: sent(moved))
        pl.when(apart)(lambda: sent(early))

    @pl.when(jnp.logical_not(lands))
    def _():
        for s in range(2):
            for a, v in pieces:

                def gone(low, s=s, a=a, v=v):
                    part = far.at[s, a, v, pl.ds(low, depth - low)]
                    pltpu.make_async_copy(part, part, far_send.at[s, a, v]).wait()

                only(apart, (a, v) in moved, functools.partial(gone, 0))
                if (a, v) == split:
                    pl.when(close)(functools.partial(gone, moving))
            for e in range(experts):
                down_pass(s, e).wait_send()

    for piece in pieces:
        a, v = piece

        def dealt(sem, a=a, v=v):
            pltpu.make_async_copy(own.at[a, v], own.at[a, v], sem).wait()

        only(close, piece in moved, lambda: crossing(a, v).wait_send())
        if piece == split:
            pl.when(apart)(lambda: crossing_part(a, v).wait_send())
        only(close, piece in early, lambda: dealt(near_send.at[a, v]))
    for e in range(experts):
        down_to(0, e).wait_send()
        down_to(1, e).wait_send()


def finish(gate_in, up_in, down_in, mixed_in, gate, up, down, mixed, ring, small, take, put, side):
    slots, rows, width = ring.shape
    steps = []
    for source, target in ((gate_in, gate), (up_in, up), (down_in, down)):
        experts, height, span = source.shape
        for e in range(experts):
            for r in range(0, height, min(height, rows)):
                for c in range(0, span, width):
                    at = (e, pl.ds(r, min(height, rows)), pl.ds(c, width))
                    steps.append((source.at[at], target.at[at], min(height, rows)))

    def pull(n):
        source, _, height = steps[n]
        slot = n % slots
        return pltpu.make_async_copy(source, ring.at[slot, pl.ds(0, height)], take.at[slot])

    def push(n):
        _, target, height = steps[n]
        slot = n % slots
        return pltpu.make_async_copy(ring.at[slot, pl.ds(0, height)], target, put.at[slot])

    ahead = slots // 2
    inward = pltpu.make_async_copy(mixed_in, small, side.at[0])
    inward.start()
    for n in range(min(ahead, len(steps))):
        pull(n).start()
    for n in range(len(steps)):
        if n + ahead < len(steps):
            if n + ahead >= slots:
                push(n + ahead - slots).wait()
            pull(n + ahead).start()
        pull(n).wait()
        push(n).start()
    inward.wait()
    outward = pltpu.make_async_copy(small, mixed, side.at[1])
    outward.start()
    for n in range(max(0, len(steps) - slots), len(steps)):
        push(n).wait()
    outward.wait()


def shards(fs_size, tp_size, tokens, norm_gain, gate_weight, up_weight, down_weight, routes, route_logit):
    experts, depth, width = gate_weight.shape
    _, units, col = down_weight.shape
    rows, features = tokens.shape
    half = jnp.bfloat16
    anywhere = pl.BlockSpec(memory_space=pl.ANY)
    vmem = pl.BlockSpec(memory_space=pltpu.VMEM)
    dma = pltpu.SemaphoreType.DMA
    block = min(units, 512)
    cuts = units // block
    blocks = experts * cuts
    special = blocks // 2 - 1
    both = width // cuts
    gate_shape = jax.ShapeDtypeStruct((experts, features, units), half)
    down_shape = jax.ShapeDtypeStruct((experts, units, features), half)
    highs, owned = fs_size // 2, rows // fs_size
    tiles = min(highs, 4)
    last = special - special // 2 + 1
    mixed_shape = jax.ShapeDtypeStruct((owned, features), half)
    gate_all, up_all, down_all, _, summed = pl.pallas_call(
        functools.partial(spread, cuts, special, fs_size, tp_size),
        out_shape=(
            gate_shape, gate_shape, down_shape,
            jax.ShapeDtypeStruct((2, 2, blocks, depth, both), half),
            mixed_shape,
        ),
        in_specs=[vmem, anywhere, vmem, vmem] + [anywhere] * 3,
        out_specs=(anywhere,) * 4 + (vmem,),
        scratch_shapes=[
            pltpu.VMEM((2, blocks, depth, both), half),
            pltpu.VMEM((experts, units, col), half),
            pltpu.VMEM((2, depth, both), jnp.float32),
            pltpu.VMEM((2, units, col), jnp.float32),
            pltpu.VMEM((rows, features), half),
            pltpu.VMEM((rows, 128), jnp.float32),
            pltpu.VMEM((rows, features), jnp.float32),
            pltpu.VMEM((last, 2, features, block), half),
            pltpu.VMEM((last, block, features), half),
            pltpu.VMEM((highs, 2, owned, features), half),
            pltpu.VMEM((highs, owned, features), half),
            pltpu.VMEM((highs, owned, features), half),
            pltpu.VMEM((highs, owned, features), half),
            dma((4,)),
        ]
        + [dma((2, blocks)), dma((2, 2, blocks))]
        + [dma((2, blocks))] * 2
        + [dma((2, 2, blocks))]
        + [dma((2, blocks))] * 3
        + [dma((4, experts)), dma((3, experts))]
        + [dma((4 + experts,)), dma((3 * last,))]
        + [dma((tiles, 2))] * 2
        + [dma((highs, 2))] * 2,
        compiler_params=pltpu.CompilerParams(
            has_side_effects=True, vmem_limit_bytes=VMEM_LIMIT, collective_id=0
        ),
        name="spread",
    )(norm_gain[None, :], tokens, routes.T, route_logit.T, gate_weight, up_weight, down_weight)

    slots = 8
    gate_out, up_out, down_out, mixed = pl.pallas_call(
        finish,
        out_shape=(gate_shape, gate_shape, down_shape, mixed_shape),
        in_specs=[anywhere] * 4,
        out_specs=(anywhere,) * 4,
        scratch_shapes=[
            pltpu.VMEM((slots, features, units), half),
            pltpu.VMEM((owned, features), half),
            dma((slots,)), dma((slots,)), dma((2,)),
        ],
        compiler_params=pltpu.CompilerParams(vmem_limit_bytes=VMEM_LIMIT),
        name="finish",
    )(gate_all, up_all, down_all, summed)
    return (gate_out, up_out, down_out, mixed)


def solution(mesh):
    return jax.shard_map(
        functools.partial(shards, mesh.shape["fs"], mesh.shape["tp"]),
        mesh=mesh,
        in_specs=(
            P("tp", None),
            P("fs"),
            P(None, "fs", "tp"),
            P(None, "fs", "tp"),
            P(None, "fs", "tp"),
            P("tp", None),
            P("tp", None),
        ),
        out_specs=(
            P(None, None, "fs"),
            P(None, None, "fs"),
            P(None, "fs", None),
            P(("tp", "fs"), None),
        ),
        check_vma=False,
    )
```

```python
import functools

import jax
import jax.numpy as jnp
from jax import lax
from jax.experimental import pallas as pl
from jax.experimental.pallas import tpu as pltpu
from jax.sharding import PartitionSpec as P

EPS = 0.5
QUARTERS = 1
MESH = pl.DeviceIdType.MESH
VMEM_LIMIT = 63 * 1024 * 1024


def expert_tile(x, weight, wide, tall, total, expert, at):
    mine = x[at, :]
    gate_val = jnp.dot(mine, wide[0], preferred_element_type=jnp.float32)
    up_val = jnp.dot(mine, wide[1], preferred_element_type=jnp.float32)
    hidden = (jax.nn.silu(gate_val) * up_val).astype(jnp.bfloat16)
    result = jnp.dot(hidden, tall[...], preferred_element_type=jnp.float32)
    shares = weight[at, :]
    lane = lax.broadcasted_iota(jnp.int32, shares.shape, 1)
    share = jnp.sum(jnp.where(lane == expert, shares, 0.0), axis=1, keepdims=True)
    total[at, :] += share * result


def expert_rows(x, weight, wide, tall, total, expert):
    rows = x.shape[0]
    tile = rows // 2

    def step(i, carry):
        at = pl.ds(pl.multiple_of(i * tile, tile), tile)
        expert_tile(x, weight, wide, tall, total, expert, at)
        return carry

    lax.fori_loop(0, rows // tile, step, 0)


def spread(
    cuts, special, fs_size, tp_size,
    gain, tokens, routes, logit, gate_f32, up_f32, down_f32,
    gate_all, up_all, down_all, far, mixed,
    own, down, stage, down_stage, x, weight, total, wide, tall, part, low_in, mid, high_in,
    load, across_send, across_recv, near_send, near_recv, far_send, twin_send, twin_recv,
    onward_send, down_send, down_recv, local_sem, fetch_sem,
    low_send, low_recv, high_send, high_recv,
):
    _, blocks, depth, both = own.shape
    experts = blocks // cuts
    features, units = gate_all.shape[1:]
    block = units // cuts
    per = both // block
    fs, tp = lax.axis_index("fs"), lax.axis_index("tp")
    half, side = tp // 2, tp % 2
    twin = half * 2 + 1 - side
    col = down.shape[2]
    group = fs // per
    relay_side = group % 2
    lands = side != relay_side
    beyond = (1 - half) * 2
    apart = group // 2 != half
    close = group // 2 == half
    full = (gate_all, up_all)

    def remote(src, dst, send, recv, fs_to, tp_to):
        return pltpu.make_async_remote_copy(
            src_ref=src, dst_ref=dst, send_sem=send, recv_sem=recv,
            device_id=(fs_to, tp_to), device_id_type=MESH,
        )

    def columns(owner):
        return pl.ds(pl.multiple_of(owner * col, col), col)

    def slab(v):
        return v // cuts, pl.ds(pl.multiple_of(v % cuts * block, block), block)

    def only(condition, needed, action):
        if needed:
            pl.when(condition)(action)
        else:
            action()

    lead = [(a, v) for v in range(special) for a in range(2)]
    early, late = lead[:special], lead[special:]
    split, final = (0, blocks - 1), (1, blocks - 1)
    lead.append(split)
    middle = [(a, v) for v in range(special, blocks - 1) for a in range(2)]
    pieces = lead + middle + [final]
    ahead = list(range(special // cuts))
    after = {}
    for e in range(experts):
        inside = [n for n, (a, v) in enumerate(pieces[:-1]) if v // cuts == e and (a, v) in middle]
        after.setdefault(inside[-1] if inside else len(pieces) - 1, []).append(e)
    for e in ahead:
        after = {n: [i for i in held if i != e] for n, held in after.items()}
        after.setdefault(2 * cuts * (e + 1) - 1, []).append(e)
    moving = depth * QUARTERS // 4
    kept = pl.ds(moving, depth - moving)

    def crossing(a, v):
        return remote(
            own.at[a, v], far.at[side, a, v], across_send.at[a, v], across_recv.at[side, a, v],
            fs, beyond + relay_side,
        )

    def crossing_part(a, v):
        return remote(
            own.at[a, v, kept], far.at[side, a, v, kept], across_send.at[a, v],
            across_recv.at[side, a, v], fs, beyond + relay_side,
        )

    def deal(source, a, v, owner, sem, low=0):
        e, at = slab(v)
        rows = pl.ds(pl.multiple_of(fs * depth + low, low or depth), depth - low)
        for h in range(per):
            remote(
                source.at[:, pl.ds(h * block, block)],
                full[a].at[e, rows, at],
                sem,
                near_recv.at[a, v],
                owner * per + h,
                half * 2 + 1 - owner % 2,
            ).start()

    def fetch(n):
        a, v = pieces[n]
        for h in range(per):
            pltpu.make_async_copy(
                (gate_f32, up_f32)[a].at[
                    v // cuts, :, pl.ds(h * units + v % cuts * block, block)
                ],
                stage.at[n % 2, :, pl.ds(h * block, block)],
                load.at[n % 2],
            ).start()

    def fetched(n):
        pltpu.make_async_copy(stage.at[n % 2], stage.at[n % 2], load.at[n % 2]).wait()

    def fetch_down(e):
        return pltpu.make_async_copy(down_f32.at[e], down_stage.at[e % 2], load.at[2 + e % 2])

    def down_local(e):
        return pltpu.make_async_copy(
            down.at[e], down_all.at[e, :, columns(tp)], local_sem.at[4 + e]
        )

    def down_to(k, e):
        return remote(
            down.at[e], down_all.at[e, :, columns(tp)], down_send.at[k, e],
            down_recv.at[(0, 1 + side)[k], e], fs, (twin, beyond + relay_side)[k],
        )

    def down_pass(s, e):
        part = down_all.at[e, :, columns(beyond + s)]
        return remote(part, part, down_send.at[2 + s, e], down_recv.at[1 + s, e], fs, twin)

    def relay(a, v, low=0):
        for s in range(2):
            part = far.at[s, a, v, pl.ds(low, depth - low)]
            pltpu.make_async_copy(part, part, across_recv.at[s, a, v]).wait()
            deal(part, a, v, beyond + s, far_send.at[s, a, v], low)

    met = pltpu.get_barrier_semaphore()

    def greet():
        def signal(i, carry):
            to = lax.rem(fs * tp_size + tp + i, fs_size * tp_size)
            pl.semaphore_signal(
                met, inc=1, device_id=(to // tp_size, to % tp_size), device_id_type=MESH
            )
            return carry

        lax.fori_loop(1, fs_size * tp_size, signal, 0)

    def meet():
        pl.semaphore_wait(met, fs_size * tp_size - 1)

    turns = {len(pieces) // 2 + 3 * i: piece for i, piece in enumerate(early)}

    tile = min(depth, 32)
    greet()
    fetch(0)
    token_copy = pltpu.make_async_copy(tokens, x, local_sem.at[0])
    token_copy.start()
    spot = lax.broadcasted_iota(jnp.int32, (depth, depth), 0)
    lane = lax.broadcasted_iota(jnp.int32, (depth, depth), 1)
    factor = jnp.sum(jnp.where(spot == lane, gain[...], 0.0), axis=1, keepdims=True)
    weight[0:depth, :] = jnp.broadcast_to(factor, (depth, weight.shape[1]))
    for n, piece in enumerate(pieces):
        a, v = piece
        if n + 1 < len(pieces):
            fetch(n + 1)
        if n == 0:
            fetch_down(0).start()
            fetch_down(1).start()
        fetched(n)
        if n == 0:
            meet()

        def scale(i, carry, a=a, v=v, n=n):
            at = pl.ds(pl.multiple_of(i * tile, tile), tile)
            own[a, v, at, :] = (stage[n % 2, at, :] * weight[at, 0:1]).astype(own.dtype)
            return carry

        lax.fori_loop(0, depth // tile, scale, 0)
        only(close, piece in late or piece == split, lambda: crossing(a, v).start())
        if piece == split:
            pl.when(apart)(lambda: crossing_part(a, v).start())
        only(close, piece in early, lambda: deal(own.at[a, v], a, v, tp, near_send.at[a, v]))
        for e in after.get(n, []):
            fetch_down(e).wait()
            short = min(units, 128)

            def narrow(i, carry, e=e):
                at = pl.ds(pl.multiple_of(i * short, short), short)
                down[e, at, :] = down_stage[e % 2, at, :].astype(down.dtype)
                return carry

            lax.fori_loop(0, units // short, narrow, 0)
            if e + 2 < experts:
                fetch_down(e + 2).start()
            down_to(1, e).start()
            down_to(0, e).start()
            down_local(e).start()
        if n in turns:
            pl.when(jnp.logical_not(lands))(functools.partial(relay, *turns[n]))
    for n, piece in turns.items():
        if n >= len(pieces):
            pl.when(jnp.logical_not(lands))(functools.partial(relay, *piece))

    token_copy.wait()
    count = x.shape[0]
    strip = count // 8

    def normalise(i, carry):
        at = pl.ds(pl.multiple_of(i * strip, strip), strip)
        floats = x[at, :].astype(jnp.float32)
        x[at, :] = (
            floats * lax.rsqrt(jnp.mean(floats * floats, axis=1, keepdims=True) + EPS)
        ).astype(x.dtype)
        return carry

    lax.fori_loop(0, count // strip, normalise, 0)
    first = jax.nn.sigmoid(logit[0:1, :] - logit[1:2, :])
    expert_of = lax.broadcasted_iota(jnp.int32, (weight.shape[1], count), 0)
    by_expert = jnp.where(routes[0:1, :] == expert_of, first, 0.0) + jnp.where(
        routes[1:2, :] == expert_of, 1.0 - first, 0.0
    )
    weight[...] = by_expert.T
    total[...] = jnp.zeros_like(total)

    def relay_down(e):
        for s in range(2):
            down_pass(s, e).wait_recv()
            down_pass(s, e).start()

    away = pl.ds(pl.multiple_of((1 - group // 2) * (features // 2), features // 2), features // 2)

    def hand(a, v):
        e, at = slab(v)
        part = full[a].at[e, :, at]
        return remote(part, part, twin_send.at[a, v], twin_recv.at[a, v], fs, twin)

    sources = features // depth // 2

    def onward(a, v):
        e, at = slab(v)
        if (a, v) != split:
            part = full[a].at[e, away, at]
            remote(
                part, part, onward_send.at[a, v], near_recv.at[a, v], fs, beyond + side
            ).start()
        else:

            def send(i, carry):
                start = ((1 - group // 2) * sources + i) * depth
                part = full[a].at[e, pl.ds(pl.multiple_of(start, depth), moving), at]
                remote(
                    part, part, onward_send.at[a, v], near_recv.at[a, v], fs, beyond + side
                ).start()
                return carry

            lax.fori_loop(0, sources, send, 0)

    def onward_sent(a, v):
        e, at = slab(v)
        count = sources * (moving if (a, v) == split else depth)
        part = full[a].at[e, pl.ds(0, count), at]
        pltpu.make_async_copy(part, part, onward_send.at[a, v]).wait()

    def take(a, v, forward):
        e, at = slab(v)
        part = full[a].at[e, :, at]
        pltpu.make_async_copy(part, part, near_recv.at[a, v]).wait()
        if forward:
            onward(a, v)
        hand(a, v).start()

    def take_all(group_of, forward):
        for a, v in group_of:
            take(a, v, forward)

    @pl.when(jnp.logical_not(lands))
    def _():
        for n, (a, v) in enumerate(lead):
            if (a, v) not in early:
                pl.when(apart)(functools.partial(relay, a, v))
            if (a, v) == split:
                pl.when(close)(functools.partial(relay, a, v, moving))
            for e in after.get(n, []):
                relay_down(e)

    moved = late + [split]

    @pl.when(lands)
    def _():
        pl.when(close)(lambda: take_all(moved, True))
        pl.when(apart)(lambda: take_all(early, True))

    def arrive(v):
        @pl.when(lands)
        def _():
            take(0, v, False)
            take(1, v, False)

        @pl.when(jnp.logical_not(lands))
        def _():
            hand(0, v).wait_recv()
            hand(1, v).wait_recv()

    def down_ready(e):
        down_local(e).wait()
        down_to(0, e).wait_recv()

        @pl.when(lands)
        def _():
            for s in range(2):
                down_pass(s, e).wait_recv()

    def bring(a, v, i):
        e, at = slab(v)
        return pltpu.make_async_copy(full[a].at[e, :, at], wide.at[i, a], fetch_sem.at[3 * i + a])

    def bring_down(v, i):
        e, at = slab(v)
        return pltpu.make_async_copy(down_all.at[e, at, :], tall.at[i], fetch_sem.at[3 * i + 2])

    def compute(v):
        e, at = slab(v)
        copies = [bring(0, v, 0), bring(1, v, 0), bring_down(v, 0)]
        for copy in copies:
            copy.start()
        for copy in copies:
            copy.wait()
        expert_rows(x, weight, wide.at[0], tall.at[0], total, e)

    for e in range(special // cuts):
        down_ready(e)

    def pass_on(v):
        @pl.when(v < blocks - 1)
        def _():
            relay(0, v)
            relay(1, v)
            last = jnp.logical_or(v % cuts == cuts - 1, v == blocks - 2)
            pl.when(last)(lambda: relay_down(v // cuts))

        @pl.when(v == blocks - 1)
        def _():
            relay(*final)
            for e in after.get(len(pieces) - 1, []):
                relay_down(e)

    def turn(v, carry):
        pl.when(jnp.logical_not(lands))(lambda: pass_on(v))

        @pl.when(v >= special + lag)
        def _():
            w = v - lag
            arrive(w)
            pl.when(jnp.logical_or(w % cuts == 0, w == special))(lambda: down_ready(w // cuts))
            compute(w)

        return carry

    lag = 2
    lax.fori_loop(special, blocks, turn, 0)

    @pl.when(jnp.logical_and(lands, close))
    def _():
        take_all(early, False)

    for v in range(special // 2):

        @pl.when(jnp.logical_not(lands))
        def _(v=v):
            hand(0, v).wait_recv()
            hand(1, v).wait_recv()

        compute(v)
    arrive(blocks - 2)
    if (blocks - 2) % cuts == 0 or blocks - 2 == special:
        down_ready((blocks - 2) // cuts)
    compute(blocks - 2)
    if (blocks - 1) // cuts != (blocks - 2) // cuts:
        down_ready(experts - 1)
    ends = list(range(special // 2, special)) + [blocks - 1]
    for i, v in enumerate(ends):
        bring_down(v, i).start()
    coming = [p for p in lead[special // 2 * 2 :] + [final]]

    @pl.when(lands)
    def _():
        for a, v in coming:
            if (a, v) in moved:
                pl.when(apart)(functools.partial(take, a, v, False))
            if (a, v) == final:
                take(a, v, False)
            bring(a, v, ends.index(v)).start()

    @pl.when(jnp.logical_not(lands))
    def _():
        for a, v in coming:
            hand(a, v).wait_recv()
            bring(a, v, ends.index(v)).start()

    for i, v in enumerate(ends):
        bring_down(v, i).wait()
        bring(0, v, i).wait()
        bring(1, v, i).wait()

    highs, _, owned, width = part.shape
    high, low = fs // 2, fs % 2
    tiles = min(highs, 4)
    held = highs // tiles
    span = count // tiles
    column = width // 2

    paired = held == 1 and tiles == 4

    def flip(value, mask):
        ones, twos = value % 2, value // 2
        low_bit = ones + mask % 2 - 2 * ones * (mask % 2)
        return low_bit + 2 * (twos + mask // 2 - 2 * twos * (mask // 2))

    def tile_of(k):
        return flip(high, tiles - k) if paired else lax.rem(high // held + k, tiles)

    def low_copy(k, c):
        t = tile_of(k)
        at, over = pl.ds(t * held, held), pl.ds(c * column, column)
        return remote(
            part.at[at, 1 - low, :, over], low_in.at[at, :, over],
            low_send.at[t, c], low_recv.at[t, c], high * 2 + 1 - low, tp,
        )

    def high_copy(shift, c):
        to = lax.rem(high + shift, highs)
        over = pl.ds(c * column, column)
        return remote(
            mid.at[to, :, over], high_in.at[shift, :, over],
            high_send.at[shift, c], high_recv.at[shift, c], to * 2 + low, tp,
        )

    def pair_copy(k, c):
        over = pl.ds(c * column, column)
        to = flip(high, 2 if k == 2 else 1)
        return remote(
            mid.at[tile_of(k), :, over], high_in.at[k, :, over],
            high_send.at[k, c], high_recv.at[k, c], to * 2 + low, tp,
        )

    def pair_merge(k):
        t = tile_of(k)
        for c in range(2):
            over = pl.ds(c * column, column)
            low_copy(k, c).wait_recv()
            sums = part[t, low, :, over].astype(jnp.float32) + low_in[t, :, over].astype(
                jnp.float32
            )
            if k == 2:
                pair_copy(1, c).wait_recv()
                sums = sums + high_in[1, :, over].astype(jnp.float32)
            mid[t, :, over] = sums.astype(mid.dtype)
            pair_copy(k, c).start()

    def merge(k):
        t = tile_of(k)
        for c in range(2):
            over = pl.ds(c * column, column)
            low_copy(k, c).wait_recv()
            for n in range(held):
                to = t * held + n
                mid[to, :, over] = (
                    part[to, low, :, over].astype(jnp.float32)
                    + low_in[to, :, over].astype(jnp.float32)
                ).astype(mid.dtype)

                @pl.when(to != high)
                def _(to=to):
                    high_copy(lax.rem(to - high + highs, highs), c).start()

    def closing(k, carry):
        t = tile_of(k)
        at = pl.ds(pl.multiple_of(t * span, span), span)
        for i, v in enumerate(ends):
            expert_tile(x, weight, wide.at[i], tall.at[i], total, v // cuts, at)
        values = total[at, :]
        for n in range(held):
            for side_of in range(2):
                start = (n * 2 + side_of) * owned
                part[t * held + n, side_of] = values[start : start + owned].astype(part.dtype)
        for c in range(2):
            low_copy(k, c).start()
        if paired:
            for step in range(1, tiles):
                pl.when(k == step + 1)(functools.partial(pair_merge, step))
        else:
            pl.when(k >= 2)(lambda: merge(k - 1))
        return carry

    lax.fori_loop(1, tiles + 1, closing, 0)
    if not paired:
        merge(tiles)
    for c in range(2):
        over = pl.ds(c * column, column)
        if paired:
            low_copy(tiles, c).wait_recv()
        gathered = part[high, low, :, over].astype(jnp.float32) + low_in[high, :, over].astype(
            jnp.float32
        )
        for shift in (2, 3) if paired else range(1, highs):
            (pair_copy if paired else high_copy)(shift, c).wait_recv()
            gathered = gathered + high_in[shift, :, over].astype(jnp.float32)
        mixed[:, over] = gathered.astype(mixed.dtype)
    for c in range(2):
        for k in range(1, tiles + 1):
            low_copy(k, c).wait_send()
        for shift in range(1, highs):
            (pair_copy if paired else high_copy)(shift, c).wait_send()

    @pl.when(lands)
    def _():
        for a, v in pieces:
            hand(a, v).wait_send()

        def sent(group_of):
            for a, v in group_of:
                onward_sent(a, v)

        pl.when(close)(lambda: sent(moved))
        pl.when(apart)(lambda: sent(early))

    @pl.when(jnp.logical_not(lands))
    def _():
        for s in range(2):
            for a, v in pieces:

                def gone(low, s=s, a=a, v=v):
                    part = far.at[s, a, v, pl.ds(low, depth - low)]
                    pltpu.make_async_copy(part, part, far_send.at[s, a, v]).wait()

                only(apart, (a, v) in moved, functools.partial(gone, 0))
                if (a, v) == split:
                    pl.when(close)(functools.partial(gone, moving))
            for e in range(experts):
                down_pass(s, e).wait_send()

    for piece in pieces:
        a, v = piece

        def dealt(sem, a=a, v=v):
            pltpu.make_async_copy(own.at[a, v], own.at[a, v], sem).wait()

        only(close, piece in moved, lambda: crossing(a, v).wait_send())
        if piece == split:
            pl.when(apart)(lambda: crossing_part(a, v).wait_send())
        only(close, piece in early, lambda: dealt(near_send.at[a, v]))
    for e in range(experts):
        down_to(0, e).wait_send()
        down_to(1, e).wait_send()


def finish(gate_in, up_in, down_in, mixed_in, gate, up, down, mixed, ring, small, take, put, side):
    slots, rows, width = ring.shape
    steps = []
    for source, target in ((gate_in, gate), (up_in, up), (down_in, down)):
        experts, height, span = source.shape
        for e in range(experts):
            for r in range(0, height, min(height, rows)):
                for c in range(0, span, width):
                    at = (e, pl.ds(r, min(height, rows)), pl.ds(c, width))
                    steps.append((source.at[at], target.at[at], min(height, rows)))

    def pull(n):
        source, _, height = steps[n]
        slot = n % slots
        return pltpu.make_async_copy(source, ring.at[slot, pl.ds(0, height)], take.at[slot])

    def push(n):
        _, target, height = steps[n]
        slot = n % slots
        return pltpu.make_async_copy(ring.at[slot, pl.ds(0, height)], target, put.at[slot])

    ahead = slots // 2
    inward = pltpu.make_async_copy(mixed_in, small, side.at[0])
    inward.start()
    for n in range(min(ahead, len(steps))):
        pull(n).start()
    for n in range(len(steps)):
        if n + ahead < len(steps):
            if n + ahead >= slots:
                push(n + ahead - slots).wait()
            pull(n + ahead).start()
        pull(n).wait()
        push(n).start()
    inward.wait()
    outward = pltpu.make_async_copy(small, mixed, side.at[1])
    outward.start()
    for n in range(max(0, len(steps) - slots), len(steps)):
        push(n).wait()
    outward.wait()


def shards(fs_size, tp_size, tokens, norm_gain, gate_weight, up_weight, down_weight, routes, route_logit):
    experts, depth, width = gate_weight.shape
    _, units, col = down_weight.shape
    rows, features = tokens.shape
    half = jnp.bfloat16
    anywhere = pl.BlockSpec(memory_space=pl.ANY)
    vmem = pl.BlockSpec(memory_space=pltpu.VMEM)
    dma = pltpu.SemaphoreType.DMA
    block = min(units, 512)
    cuts = units // block
    blocks = experts * cuts
    special = blocks // 2 - 1
    both = width // cuts
    gate_shape = jax.ShapeDtypeStruct((experts, features, units), half)
    down_shape = jax.ShapeDtypeStruct((experts, units, features), half)
    highs, owned = fs_size // 2, rows // fs_size
    tiles = min(highs, 4)
    last = special - special // 2 + 1
    mixed_shape = jax.ShapeDtypeStruct((owned, features), half)
    gate_all, up_all, down_all, _, summed = pl.pallas_call(
        functools.partial(spread, cuts, special, fs_size, tp_size),
        out_shape=(
            gate_shape, gate_shape, down_shape,
            jax.ShapeDtypeStruct((2, 2, blocks, depth, both), half),
            mixed_shape,
        ),
        in_specs=[vmem, anywhere, vmem, vmem] + [anywhere] * 3,
        out_specs=(anywhere,) * 4 + (vmem,),
        scratch_shapes=[
            pltpu.VMEM((2, blocks, depth, both), half),
            pltpu.VMEM((experts, units, col), half),
            pltpu.VMEM((2, depth, both), jnp.float32),
            pltpu.VMEM((2, units, col), jnp.float32),
            pltpu.VMEM((rows, features), half),
            pltpu.VMEM((rows, 128), jnp.float32),
            pltpu.VMEM((rows, features), jnp.float32),
            pltpu.VMEM((last, 2, features, block), half),
            pltpu.VMEM((last, block, features), half),
            pltpu.VMEM((highs, 2, owned, features), half),
            pltpu.VMEM((highs, owned, features), half),
            pltpu.VMEM((highs, owned, features), half),
            pltpu.VMEM((highs, owned, features), half),
            dma((4,)),
        ]
        + [dma((2, blocks)), dma((2, 2, blocks))]
        + [dma((2, blocks))] * 2
        + [dma((2, 2, blocks))]
        + [dma((2, blocks))] * 3
        + [dma((4, experts)), dma((3, experts))]
        + [dma((4 + experts,)), dma((3 * last,))]
        + [dma((tiles, 2))] * 2
        + [dma((highs, 2))] * 2,
        compiler_params=pltpu.CompilerParams(
            has_side_effects=True, vmem_limit_bytes=VMEM_LIMIT, collective_id=0
        ),
        name="spread",
    )(norm_gain[None, :], tokens, routes.T, route_logit.T, gate_weight, up_weight, down_weight)

    slots = 8
    gate_out, up_out, down_out, mixed = pl.pallas_call(
        finish,
        out_shape=(gate_shape, gate_shape, down_shape, mixed_shape),
        in_specs=[anywhere] * 4,
        out_specs=(anywhere,) * 4,
        scratch_shapes=[
            pltpu.VMEM((slots, features, units), half),
            pltpu.VMEM((owned, features), half),
            dma((slots,)), dma((slots,)), dma((2,)),
        ],
        compiler_params=pltpu.CompilerParams(vmem_limit_bytes=VMEM_LIMIT),
        name="finish",
    )(gate_all, up_all, down_all, summed)
    return (gate_out, up_out, down_out, mixed)


def solution(mesh):
    return jax.shard_map(
        functools.partial(shards, mesh.shape["fs"], mesh.shape["tp"]),
        mesh=mesh,
        in_specs=(
            P("tp", None),
            P("fs"),
            P(None, "fs", "tp"),
            P(None, "fs", "tp"),
            P(None, "fs", "tp"),
            P("tp", None),
            P("tp", None),
        ),
        out_specs=(
            P(None, None, "fs"),
            P(None, None, "fs"),
            P(None, "fs", None),
            P(("tp", "fs"), None),
        ),
        check_vma=False,
    )
```
